1024 devices in a mesh: ep: 64 (over z, y), tp: 16 (over x, core).
Axes of the slice: x: 8, y: 8, z: 8, core: 2. Of those that a mesh axis runs over, the one named last changes fastest.
Arguments:
- tokens: bfloat16 [16384, 2048], P('ep', 'tp'), may hold values from -6 to 6
- experts: int32 [16384, 16], P('ep'), may hold values from 0 to 262143, as said below
- weights: float32 [16384, 16], P('ep'), may hold values from 0.05 to 1
- up_table: bfloat16 [262144, 2048], P('ep', 'tp'), may hold values from -0.125 to 0.125
- out_table: bfloat16 [262144, 2048], P('ep', 'tp')
- gain: float32 [2048], P('tp'), may hold values from 0.1 to 1.9
Outputs:
- normed: bfloat16 [16384, 2048], P('ep', 'tp')
The draws below stay inside these ranges and needn't reach their ends.
Inputs may be any that keep to these rules, and one draw needn't show every extreme that they name: An expert number e lies with index e // 4096 of ep. Among the rows of one index of ep, at most 128 chosen experts lie with any one index of ep, and in every draw some index of ep receives exactly 128 from every index.
All inputs are finite; a program needn't handle non-finite values.
Results may differ from the reference program's by a relative error of at most 0.006.
Values may be sent and summed in bfloat16 or wider, within the bound.
A program may use at most 32 MiB of HBM per device.

```python
import math
import jax
import jax.numpy as jnp
from jax import lax

D = 2048
SLOTS = 16
EXPERTS_PER_RANK = 4096
TOK_DEV = 256
TOKENS = 16384
EXPERTS = 262144
ROW_LIMIT = 128
N_EP = 64


def draw_experts(key, part):
    request_list = TOK_DEV * SLOTS
    slot_count = N_EP * ROW_LIMIT
    order = jax.random.permutation(jax.random.fold_in(key, 11), N_EP)
    pinned_choice = (order < N_EP // 8).astype(jnp.int32)
    slot_holder_rank = jnp.arange(slot_count, dtype=jnp.int32) // ROW_LIMIT

    def one_source(sender_rank):
        score_key = jax.random.fold_in(key, sender_rank + 100)
        random_jitter = jax.random.randint(jax.random.fold_in(score_key, 1), (slot_count,), 0, 4096, dtype=jnp.int32)
        expert_score = (pinned_choice[slot_holder_rank] * 8192 + random_jitter) * slot_count + jnp.arange(slot_count, dtype=jnp.int32)
        selected_rows = lax.top_k(expert_score, request_list)[1].astype(jnp.int32)
        owner_ranks = jax.random.permutation(jax.random.fold_in(score_key, 2), selected_rows // ROW_LIMIT)
        picked_experts = jax.random.randint(jax.random.fold_in(score_key, 3), (3, request_list), 0, EXPERTS_PER_RANK, dtype=jnp.int32)
        local = picked_experts[0] * picked_experts[1] // EXPERTS_PER_RANK * picked_experts[2] // EXPERTS_PER_RANK
        return (owner_ranks * EXPERTS_PER_RANK + local).reshape(TOK_DEV, SLOTS)
    return lax.map(one_source, jnp.arange(N_EP, dtype=jnp.int32)).reshape(TOK_DEV * N_EP, SLOTS)


def draw_out_table(key, part):
    cols = jnp.arange(D, dtype=jnp.float32) / D
    jitter = jnp.exp(jax.random.uniform(jax.random.fold_in(key, 2), (D,), jnp.float32, -0.35, 0.35))
    rowscale = jnp.exp(jax.random.uniform(jax.random.fold_in(key, 3), (EXPERTS, 1), jnp.float32, 0.0, math.log(10.0)))
    base = jax.random.normal(jax.random.fold_in(key, 6), (EXPERTS, D), jnp.float32)
    colscale = 10.0 ** cols * jitter
    return (0.1 * base * rowscale * colscale[None, :]).astype(jnp.bfloat16)


def block_scale(key, extent, cuts, least, top_value):
    level, own = 1.0, jax.random.fold_in(key, 6)
    for dim, shards_of in cuts:
        steps = jnp.exp(jax.random.uniform(jax.random.fold_in(own, dim), (shards_of,), jnp.float32, least / len(cuts), top_value / len(cuts)))
        level = level * jnp.repeat(steps, extent[dim] // shards_of).reshape([-1 if axis == dim else 1 for axis in range(len(extent))])
    return level


def scatter_about(stream_key, extent, spread, most, cuts=(), kind=jnp.bfloat16):
    level = block_scale(stream_key, extent, cuts, -0.22, 0.18) if cuts else 1.0
    values = jax.random.normal(stream_key, extent, jnp.float32) * spread * level
    return jnp.minimum(jnp.maximum(values, -most), most).astype(kind)


def setup_inputs(seed: int = 0) -> dict:
    key_of = jax.random.split(jax.random.key(seed), 7)
    tokens = scatter_about(key_of[0], (TOKENS, D), 1.0, 6.0, ((0, 64), (1, 16)))
    experts = draw_experts(jax.random.fold_in(key_of[6], 71), 0)
    weights = jnp.clip(jnp.exp(math.log(1.0) - 2.9957323 * jax.random.uniform(key_of[2], (TOKENS, SLOTS), jnp.float32) ** block_scale(key_of[2], (TOKENS, SLOTS), ((0, 64),), -0.2, 0.2)), 0.05, 1.0)
    up_table = scatter_about(key_of[3], (EXPERTS, D), D ** -0.5, 0.125, ((0, 64), (1, 16)))
    out_table = draw_out_table(jax.random.fold_in(key_of[6], 71), 0)
    gain = jnp.clip(1.0 + 0.18 * jax.random.normal(key_of[5], (D,), jnp.float32), 0.1, 1.9)
    return {"tokens": tokens, "experts": experts, "weights": weights, "up_table": up_table, "out_table": out_table, "gain": gain}


def reference(tokens, experts, weights, up_table, out_table, gain):
    blocks = tokens.shape[0] // TOK_DEV
    tok_blocks = tokens.reshape(blocks, TOK_DEV, D)
    id_blocks = experts.reshape(blocks, TOK_DEV, SLOTS)
    wt_blocks = weights.reshape(blocks, TOK_DEV, SLOTS)
    gain_f = gain.astype(jnp.float32)

    def one_block(args):
        rows, ids, wts = args
        up_rows = up_table[ids].astype(jnp.float32)
        dot = jnp.einsum('tw,tkw->tk', rows.astype(jnp.float32), up_rows)
        act = jax.nn.gelu(dot)
        contrib = (act[:, :, None] * out_table[ids].astype(jnp.float32)).astype(jnp.bfloat16)
        mixed = jnp.einsum('tk,tkw->tw', wts.astype(jnp.float32), contrib.astype(jnp.float32))
        power = lax.optimization_barrier(jnp.mean(mixed * mixed, axis=1))
        return (mixed * lax.rsqrt(power + 1e-06)[:, None] * gain_f[None, :]).astype(jnp.bfloat16)
    normed = lax.map(one_block, (tok_blocks, id_blocks, wt_blocks))
    return normed.reshape(tokens.shape[0], D)
```

```python
import functools

import jax
import jax.numpy as jnp
from jax import lax
from jax.experimental import pallas as pl
from jax.experimental.pallas import tpu as pltpu
from jax.sharding import PartitionSpec as P

F32, BF16, I32 = jnp.float32, jnp.bfloat16, jnp.int32
CONTRACT_MINOR = (((1,), (1,)), ((), ()))


def bucket_kernel(rows_held, expert_ref, weight_ref, id_ref, tok_ref, wgt_ref):
    slots, toks = expert_ref.shape
    owners, cap = id_ref.shape
    shift = rows_held.bit_length() - 1
    owner_no = lax.broadcasted_iota(I32, (owners, toks), 0)
    rank_no = lax.broadcasted_iota(I32, (cap, toks), 0)
    token_no = lax.broadcasted_iota(I32, (1, toks), 1).astype(F32)
    first = lax.broadcasted_iota(I32, (toks, toks), 0)
    second = lax.broadcasted_iota(I32, (toks, toks), 1)
    earlier = jnp.where(first < second, 1.0, 0.0).astype(BF16)
    ones = jnp.ones((toks, toks), BF16)
    before = jnp.zeros((owners, toks), F32)
    found = jnp.zeros((5 * owners, cap), F32)
    for k in range(slots):
        expert = expert_ref[k : k + 1, :]
        local = expert & (rows_held - 1)
        mine = (expert >> shift) == owner_no
        onehot = jnp.where(mine, 1.0, 0.0).astype(BF16)
        rank = before + jnp.dot(onehot, earlier, preferred_element_type=F32)
        before = before + jnp.dot(onehot, ones, preferred_element_type=F32)
        rank = jnp.sum(jnp.where(mine, rank, 0.0), axis=0, keepdims=True).astype(I32)
        place = jnp.where(rank == rank_no, 1.0, 0.0).astype(BF16)
        weight = weight_ref[k : k + 1, :]
        weight_hi = weight.astype(BF16).astype(F32)
        pieces = (
            (local >> 8).astype(F32),
            (local & 255).astype(F32),
            token_no,
            weight_hi,
            weight - weight_hi,
        )
        what = jnp.concatenate([jnp.where(mine, p, 0.0).astype(BF16) for p in pieces], axis=0)
        found = found + lax.dot_general(what, place, CONTRACT_MINOR, preferred_element_type=F32)
    part = [found[i * owners : (i + 1) * owners] for i in range(5)]
    id_ref[...] = (part[0] * 256.0 + part[1]).astype(I32)
    tok_ref[...] = part[2]
    wgt_ref[...] = part[3] + part[4]


def dots_kernel(id_ref, tok_ref, feat_ref, up_ref, out_ref, dot_ref, rows_ref, table, pair):
    step = pl.program_id(0)
    held = up_ref.shape[0]
    cap = id_ref.shape[1]
    toks = feat_ref.shape[1]

    @pl.when(step == 0)
    def _():
        table[pl.ds(0, held, stride=2), :] = up_ref[...].astype(F32)
        table[pl.ds(1, held, stride=2), :] = out_ref[...].astype(F32)

    for r in range(cap):
        row = id_ref[step, r]
        pair[2 * r : 2 * r + 2, :] = table[pl.ds(pl.multiple_of(row * 2, 2), 2), :]
    up = pair[pl.ds(0, cap, stride=2), :].astype(BF16)
    rows_ref[0] = pair[pl.ds(1, cap, stride=2), :].astype(BF16)
    every = lax.dot_general(feat_ref[0], up, CONTRACT_MINOR, preferred_element_type=F32)
    token = lax.broadcasted_iota(I32, (toks, cap), 0).astype(F32)
    dot_ref[0] = jnp.sum(jnp.where(tok_ref[0] == token, every, 0.0), axis=0, keepdims=True)


def mix_kernel(tok_ref, wgt_ref, dot_ref, rows_ref, mixed_ref):
    toks = mixed_ref.shape[1]
    cap = tok_ref.shape[2]
    coef = jax.nn.gelu(dot_ref[0]) * wgt_ref[0]
    coef_hi = coef.astype(BF16).astype(F32)
    token = lax.broadcasted_iota(I32, (toks, cap), 0).astype(F32)
    here = tok_ref[0] == token
    spread = jnp.concatenate(
        [jnp.where(here, c, 0.0).astype(BF16) for c in (coef_hi, coef - coef_hi)], axis=1
    )
    rows = jnp.concatenate([rows_ref[0]] * 2, axis=0)
    mixed_ref[0] = jnp.dot(spread, rows, preferred_element_type=F32).astype(mixed_ref.dtype)


def body(tokens, experts, weights, up_table, out_table, gain):
    n_ep, n_tp = lax.axis_size("ep"), lax.axis_size("tp")
    toks, width = tokens.shape
    slots = experts.shape[1]
    held = up_table.shape[0]
    cap = 2 * toks * slots // n_ep
    listed = jax.ShapeDtypeStruct((n_ep, cap), F32)
    ids, tok, wgt = pl.pallas_call(
        functools.partial(bucket_kernel, held),
        out_shape=(jax.ShapeDtypeStruct((n_ep, cap), I32), listed, listed),
        name="bucket",
    )(experts.T, weights.T)
    exchange = functools.partial(
        lax.all_to_all, axis_name="ep", split_axis=0, concat_axis=0, tiled=True
    )
    ids = exchange(ids)
    tokwgt = exchange(jnp.stack([tok, wgt], axis=1))
    feat = lax.all_gather(tokens, "ep")
    tok, wgt = tokwgt[:, :1], tokwgt[:, 1:]
    lane = pl.BlockSpec((1, 1, cap), lambda s, *_: (s, 0, 0))
    whole = pl.BlockSpec((held, width), lambda s, *_: (0, 0))
    block = pl.BlockSpec((1, toks, width), lambda s, *_: (s, 0, 0))
    rows = pl.BlockSpec((1, cap, width), lambda s, *_: (s, 0, 0))
    dot, picked = pl.pallas_call(
        dots_kernel,
        grid_spec=pltpu.PrefetchScalarGridSpec(
            num_scalar_prefetch=1,
            grid=(n_ep,),
            in_specs=[lane, block, whole, whole],
            out_specs=[lane, rows],
            scratch_shapes=[pltpu.VMEM((2 * held, width), F32), pltpu.VMEM((2 * cap, width), F32)],
        ),
        out_shape=(
            jax.ShapeDtypeStruct((n_ep, 1, cap), F32),
            jax.ShapeDtypeStruct((n_ep, cap, width), BF16),
        ),
        name="dots",
    )(ids, tok, feat, up_table, out_table)
    dot = lax.psum(dot, "tp")
    mixed = pl.pallas_call(
        mix_kernel,
        grid=(n_ep,),
        in_specs=[lane, lane, lane, rows],
        out_specs=block,
        out_shape=jax.ShapeDtypeStruct((n_ep, toks, width), BF16),
        name="mix",
    )(tok, wgt, dot, picked)
    mixed = lax.psum_scatter(mixed, "ep", scatter_dimension=0, tiled=False).astype(F32)
    square = lax.psum(jnp.sum(mixed * mixed, axis=1), "tp")
    scale = lax.rsqrt(square / (width * n_tp) + 1e-06)
    return (mixed * scale[:, None] * gain[None, :]).astype(BF16)


def solution(mesh):
    placed = (P("ep", "tp"), P("ep", None), P("ep", None), P("ep", "tp"), P("ep", "tp"), P("tp"))
    return jax.shard_map(body, mesh=mesh, in_specs=placed, out_specs=P("ep", "tp"), check_vma=False)
```

```python
import functools

import jax
import jax.numpy as jnp
from jax import lax
from jax.experimental import pallas as pl
from jax.experimental.pallas import tpu as pltpu
from jax.sharding import PartitionSpec as P

F32, BF16, I32 = jnp.float32, jnp.bfloat16, jnp.int32
CONTRACT_MINOR = (((1,), (1,)), ((), ()))
MESH = pl.DeviceIdType.MESH
ANY = pl.BlockSpec(memory_space=pl.ANY)
VMEM = pl.BlockSpec(memory_space=pltpu.VMEM)


def distance(ring, step):
    return min(step, ring - step)


def heading(ring, step, plus):
    if step == 0:
        return 0
    if 2 * step == ring:
        return 1 if plus else -1
    return 1 if 2 * step < ring else -1


def beyond(ring, step, plus):
    out = []
    for way in (1, -1):
        after = (step + way) % ring
        if after and step in (0, after - way, (after - way) % ring):
            if heading(ring, after, plus) == way and (step == 0 or heading(ring, step, plus) == way):
                out.append(way)
    return out


def wave(ring):
    every = [(q, p) for q in range(ring) for p in range(ring)]
    far = lambda qp: (distance(ring, qp[0]) + distance(ring, qp[1]), distance(ring, qp[1]), qp)
    return sorted(every, key=far)


def neighbours(ring):
    me = lax.axis_index("ep")
    z, y = me // ring, lax.rem(me, ring)
    up = lambda k: lax.rem(k + 1, ring)
    down = lambda k: lax.rem(k + ring - 1, ring)
    return z, y, {
        (0, 1): up(z) * ring + y,
        (0, -1): down(z) * ring + y,
        (1, 1): z * ring + up(y),
        (1, -1): z * ring + down(y),
    }


def greet(near):
    barrier = pltpu.get_barrier_semaphore()
    for device in near.values():
        pl.semaphore_signal(barrier, inc=1, device_id={"ep": device}, device_id_type=MESH)
    pl.semaphore_wait(barrier, len(near))


def arrived(ref, sem):
    pltpu.make_async_copy(ref, ref, sem).wait()


def gather_kernel(ring, x_ref, all_ref, send_sem, recv_sem, load_sem):
    _, _, near = neighbours(ring)
    rows = all_ref.shape[3]
    loads = [
        pltpu.make_async_copy(x_ref.at[pl.ds(h * rows, rows)], all_ref.at[h, 0, 0], load_sem.at[h])
        for h in range(2)
    ]
    for load in loads:
        load.start()
    greet(near)
    for load in loads:
        load.wait()
    sent = []

    def send(h, q, p, axis, way):
        after = ((q + way) % ring, p) if axis == h else (q, (p + way) % ring)
        copy = pltpu.make_async_remote_copy(
            all_ref.at[h, q, p],
            all_ref.at[h, *after],
            send_sem.at[len(sent)],
            recv_sem.at[h, *after],
            device_id={"ep": near[axis, way]},
            device_id_type=MESH,
        )
        copy.start()
        sent.append(copy)

    for q, p in wave(ring):
        for h in range(2):
            if (q, p) != (0, 0):
                arrived(all_ref.at[h, q, p], recv_sem.at[h, q, p])
            if p == 0:
                for way in beyond(ring, q, h == 0):
                    send(h, q, p, h, way)
            for way in beyond(ring, p, q % 2 == 0):
                send(h, q, p, 1 - h, way)
    for copy in sent:
        copy.wait_send()


def bucket_kernel(rows_held, expert_ref, weight_ref, id_ref, tok_ref, wgt_ref):
    slots, toks = expert_ref.shape
    owners, cap = id_ref.shape
    shift = rows_held.bit_length() - 1
    owner_no = lax.broadcasted_iota(I32, (owners, toks), 0)
    rank_no = lax.broadcasted_iota(I32, (cap, toks), 0)
    token_no = lax.broadcasted_iota(I32, (1, toks), 1).astype(F32)
    first = lax.broadcasted_iota(I32, (toks, toks), 0)
    second = lax.broadcasted_iota(I32, (toks, toks), 1)
    earlier = jnp.where(first < second, 1.0, 0.0).astype(BF16)
    ones = jnp.ones((toks, toks), BF16)
    before = jnp.zeros((owners, toks), F32)
    found = jnp.zeros((5 * owners, cap), F32)
    for k in range(slots):
        expert = expert_ref[k : k + 1, :]
        local = expert & (rows_held - 1)
        mine = (expert >> shift) == owner_no
        onehot = jnp.where(mine, 1.0, 0.0).astype(BF16)
        rank = before + jnp.dot(onehot, earlier, preferred_element_type=F32)
        before = before + jnp.dot(onehot, ones, preferred_element_type=F32)
        rank = jnp.sum(jnp.where(mine, rank, 0.0), axis=0, keepdims=True).astype(I32)
        place = jnp.where(rank == rank_no, 1.0, 0.0).astype(BF16)
        weight = weight_ref[k : k + 1, :]
        weight_hi = weight.astype(BF16).astype(F32)
        pieces = (
            (local >> 8).astype(F32),
            (local & 255).astype(F32),
            token_no,
            weight_hi,
            weight - weight_hi,
        )
        what = jnp.concatenate([jnp.where(mine, p, 0.0).astype(BF16) for p in pieces], axis=0)
        found = found + lax.dot_general(what, place, CONTRACT_MINOR, preferred_element_type=F32)
    part = [found[i * owners : (i + 1) * owners] for i in range(5)]
    id_ref[...] = (part[0] * 256.0 + part[1]).astype(I32)
    tok_ref[...] = part[2]
    wgt_ref[...] = part[3] + part[4]


def dots_kernel(id_ref, tok_ref, feat_a, feat_b, up_ref, out_ref, dot_ref, rows_ref, table, pair):
    step = pl.program_id(0)
    held = up_ref.shape[0]
    cap = id_ref.shape[1]
    half = feat_a.shape[3]

    @pl.when(step == 0)
    def _():
        table[pl.ds(0, held, stride=2), :] = up_ref[...].astype(F32)
        table[pl.ds(1, held, stride=2), :] = out_ref[...].astype(F32)

    for r in range(cap):
        row = id_ref[step, r]
        pair[2 * r : 2 * r + 2, :] = table[pl.ds(pl.multiple_of(row * 2, 2), 2), :]
    up = pair[pl.ds(0, cap, stride=2), :].astype(BF16)
    rows_ref[0] = pair[pl.ds(1, cap, stride=2), :].astype(BF16)
    token = lax.broadcasted_iota(I32, (half, cap), 0).astype(F32)
    total = jnp.zeros((1, cap), F32)
    for h, feat in enumerate((feat_a, feat_b)):
        every = lax.dot_general(feat[0, 0, 0], up, CONTRACT_MINOR, preferred_element_type=F32)
        here = tok_ref[0] - float(h * half) == token
        total = total + jnp.sum(jnp.where(here, every, 0.0), axis=0, keepdims=True)
    dot_ref[0] = total


def reduce_kernel(ring, tok_ref, coef_ref, rows_ref, mixed_ref, part, inbox, extra, inbox2, outbox, send_sem, recv_sem):
    z, y, near = neighbours(ring)
    toks = part.shape[1]
    rows = toks // 2
    cap = tok_ref.shape[2]
    greet(near)
    token = lax.broadcasted_iota(I32, (toks, cap), 0).astype(F32)

    def one(s, carry):
        q, p = s // ring, lax.rem(s, ring)
        source = lax.rem(z + ring - q, ring) * ring + lax.rem(y + ring - p, ring)
        here = tok_ref[source] == token
        coef = coef_ref[source]
        coef_hi = coef.astype(BF16).astype(F32)
        spread = jnp.concatenate(
            [jnp.where(here, c, 0.0).astype(BF16) for c in (coef_hi, coef - coef_hi)], axis=1
        )
        picked = rows_ref[source]
        both = jnp.concatenate([picked, picked], axis=0)
        part[s] = jnp.dot(spread, both, preferred_element_type=F32)
        return carry

    lax.fori_loop(0, ring * ring, one, 0)
    sent = []

    def send(h, q, p, value, target, slot, axis, way):
        outbox[h, q, p] = value.astype(BF16)
        copy = pltpu.make_async_remote_copy(
            outbox.at[h, q, p],
            target,
            send_sem.at[len(sent)],
            recv_sem.at[slot],
            device_id={"ep": near[axis, way]},
            device_id_type=MESH,
        )
        copy.start()
        sent.append(copy)

    number = {}

    def slot_of(*key):
        return number.setdefault(key, len(number))

    def box(h, q, p, way):
        return (extra.at[h, q], slot_of("x", h, q)) if p == 0 and way < 0 else (inbox.at[h, q, p], slot_of("i", h, q, p))

    def box2(h, q, way):
        return (inbox2.at[h, ring], slot_of("x2", h)) if q == 0 and way < 0 else (inbox2.at[h, q], slot_of("i2", h, q))

    for q, p in reversed(wave(ring)):
        for h in range(2):
            u, v = (q, p) if h == 0 else (p, q)
            value = part[u * ring + v, h * rows : (h + 1) * rows]
            plus = q % 2 == 0
            for way in beyond(ring, p, plus):
                ref, slot = box(h, q, p, way)
                arrived(ref, recv_sem.at[slot])
                value = value + ref[...].astype(F32)
            if p:
                way = heading(ring, p, plus)
                ref, slot = box(h, q, (p - way) % ring, way)
                send(h, q, p, value, ref, slot, 1 - h, -way)
                continue
            for way in beyond(ring, q, h == 0):
                ref, slot = box2(h, q, way)
                arrived(ref, recv_sem.at[slot])
                value = value + ref[...].astype(F32)
            if q:
                way = heading(ring, q, h == 0)
                ref, slot = box2(h, (q - way) % ring, way)
                send(h, q, p, value, ref, slot, h, -way)
                continue
            mixed_ref[h * rows : (h + 1) * rows, :] = value
    for copy in sent:
        copy.wait_send()


def body(tokens, experts, weights, up_table, out_table, gain):
    n_ep, n_tp = lax.axis_size("ep"), lax.axis_size("tp")
    ring = round(n_ep**0.5)
    toks, width = tokens.shape
    slots = experts.shape[1]
    held = up_table.shape[0]
    cap = 2 * toks * slots // n_ep
    half = toks // 2
    z, y, _ = neighbours(ring)
    listed = jax.ShapeDtypeStruct((n_ep, cap), F32)
    ids, tok, wgt = pl.pallas_call(
        functools.partial(bucket_kernel, held),
        out_shape=(jax.ShapeDtypeStruct((n_ep, cap), I32), listed, listed),
        name="bucket",
    )(experts.T, weights.T)
    exchange = functools.partial(
        lax.all_to_all, axis_name="ep", split_axis=0, concat_axis=0, tiled=True
    )
    ids = exchange(ids)
    tokwgt = exchange(jnp.stack([tok, wgt], axis=1))
    feat = pl.pallas_call(
        functools.partial(gather_kernel, ring),
        out_shape=jax.ShapeDtypeStruct((2, ring, ring, half, width), BF16),
        in_specs=[ANY],
        out_specs=VMEM,
        scratch_shapes=[
            pltpu.SemaphoreType.DMA((2 * (n_ep - 1),)),
            pltpu.SemaphoreType.DMA((2, ring, ring)),
            pltpu.SemaphoreType.DMA((2,)),
        ],
        compiler_params=pltpu.CompilerParams(collective_id=0, has_side_effects=True),
        name="gather",
    )(tokens)
    tok, wgt = tokwgt[:, :1], tokwgt[:, 1:]

    def turn(s, me_z, me_y):
        return lax.rem(me_z + ring - s // ring, ring) , lax.rem(me_y + ring - lax.rem(s, ring), ring)

    place = jnp.stack([z, y]).astype(I32)
    lane = pl.BlockSpec((1, 1, cap), lambda s, *_: (s, 0, 0))
    whole = pl.BlockSpec((held, width), lambda s, *_: (0, 0))
    feat_a = pl.BlockSpec((1, 1, 1, half, width), lambda s, ids, pos: (0, *turn(s, pos[0], pos[1]), 0, 0))
    feat_b = pl.BlockSpec((1, 1, 1, half, width), lambda s, ids, pos: (1, *turn(s, pos[0], pos[1])[::-1], 0, 0))
    rows = pl.BlockSpec((1, cap, width), lambda s, *_: (s, 0, 0))
    dot, picked = pl.pallas_call(
        lambda ids, pos, *refs: dots_kernel(ids, *refs),
        grid_spec=pltpu.PrefetchScalarGridSpec(
            num_scalar_prefetch=2,
            grid=(n_ep,),
            in_specs=[lane, feat_a, feat_b, whole, whole],
            out_specs=[lane, rows],
            scratch_shapes=[pltpu.VMEM((2 * held, width), F32), pltpu.VMEM((2 * cap, width), F32)],
        ),
        out_shape=(
            jax.ShapeDtypeStruct((n_ep, 1, cap), F32),
            jax.ShapeDtypeStruct((n_ep, cap, width), BF16),
        ),
        name="dots",
    )(ids, place, tok, feat, feat, up_table, out_table)
    dot = lax.psum(dot, "tp")
    coef = jax.nn.gelu(dot) * wgt
    messages = 2 * (n_ep - 1)
    mixed = pl.pallas_call(
        functools.partial(reduce_kernel, ring),
        out_shape=jax.ShapeDtypeStruct((toks, width), F32),
        in_specs=[VMEM] * 3,
        out_specs=VMEM,
        scratch_shapes=[
            pltpu.VMEM((n_ep, toks, width), F32),
            pltpu.VMEM((2, ring, ring, half, width), BF16),
            pltpu.VMEM((2, ring, half, width), BF16),
            pltpu.VMEM((2, ring + 1, half, width), BF16),
            pltpu.VMEM((2, ring, ring, half, width), BF16),
            pltpu.SemaphoreType.DMA((messages,)),
            pltpu.SemaphoreType.DMA((messages,)),
        ],
        compiler_params=pltpu.CompilerParams(collective_id=1, has_side_effects=True),
        name="reduce",
    )(tok, coef, picked)
    square = lax.psum(jnp.sum(mixed * mixed, axis=1), "tp")
    scale = lax.rsqrt(square / (width * n_tp) + 1e-06)
    return (mixed * scale[:, None] * gain[None, :]).astype(BF16)


def solution(mesh):
    placed = (P("ep", "tp"), P("ep", None), P("ep", None), P("ep", "tp"), P("ep", "tp"), P("tp"))
    return jax.shard_map(body, mesh=mesh, in_specs=placed, out_specs=P("ep", "tp"), check_vma=False)
```

```python
import functools

import jax
import jax.numpy as jnp
from jax import lax
from jax.experimental import pallas as pl
from jax.experimental.pallas import tpu as pltpu
from jax.sharding import PartitionSpec as P

F32, BF16, I32 = jnp.float32, jnp.bfloat16, jnp.int32
CONTRACT_MINOR = (((1,), (1,)), ((), ()))
MESH = pl.DeviceIdType.MESH
BATCHES = 4
GATHERS = 4
MIXES = 8


def distance(ring, step):
    return min(step, ring - step)


def heading(ring, step, plus):
    if step == 0:
        return 0
    if 2 * step == ring:
        return 1 if plus else -1
    return 1 if 2 * step < ring else -1


def beyond(ring, step, plus):
    out = []
    for way in (1, -1):
        after = (step + way) % ring
        if after and heading(ring, after, plus) == way and (step == 0 or heading(ring, step, plus) == way):
            out.append(way)
    return out


def wave(ring):
    every = [(u, v) for u in range(ring) for v in range(ring)]
    return sorted(every, key=lambda uv: (-distance(ring, uv[0]) - distance(ring, uv[1]), uv))


def arrived(ref, sem):
    pltpu.make_async_copy(ref, ref, sem).wait()


def bucket_kernel(rows_held, expert_ref, weight_ref, code_ref, share_ref):
    slots, toks = expert_ref.shape
    ring, _, cap = code_ref.shape
    owners = ring * ring
    shift = rows_held.bit_length() - 1
    owner_no = lax.broadcasted_iota(I32, (owners, toks), 0)
    rank_no = lax.broadcasted_iota(I32, (cap, toks), 0)
    token_no = lax.broadcasted_iota(I32, (1, toks), 1).astype(F32)
    first = lax.broadcasted_iota(I32, (toks, toks), 0)
    second = lax.broadcasted_iota(I32, (toks, toks), 1)
    earlier = jnp.where(first < second, 1.0, 0.0).astype(BF16)
    ones = jnp.ones((toks, toks), BF16)
    before = jnp.zeros((owners, toks), F32)
    found = jnp.zeros((5 * owners, cap), F32)
    for k in range(slots):
        expert = expert_ref[k : k + 1, :]
        local = expert & (rows_held - 1)
        mine = (expert >> shift) == owner_no
        onehot = jnp.where(mine, 1.0, 0.0).astype(BF16)
        rank = before + jnp.dot(onehot, earlier, preferred_element_type=F32)
        before = before + jnp.dot(onehot, ones, preferred_element_type=F32)
        rank = jnp.sum(jnp.where(mine, rank, 0.0), axis=0, keepdims=True).astype(I32)
        place = jnp.where(rank == rank_no, 1.0, 0.0).astype(BF16)
        weight = weight_ref[k : k + 1, :]
        weight_hi = weight.astype(BF16).astype(F32)
        pieces = (
            (local >> 8).astype(F32),
            (local & 255).astype(F32),
            token_no,
            weight_hi,
            weight - weight_hi,
        )
        what = jnp.concatenate([jnp.where(mine, p, 0.0).astype(BF16) for p in pieces], axis=0)
        found = found + lax.dot_general(what, place, CONTRACT_MINOR, preferred_element_type=F32)
    part = [found[i * owners : (i + 1) * owners] for i in range(5)]
    code = part[2] * float(rows_held) + part[0] * 256.0 + part[1]
    weight = part[3] + part[4]
    for k in range(ring):
        code_ref[k] = code[k * ring : (k + 1) * ring].astype(I32)
        share_ref[k] = weight[k * ring : (k + 1) * ring]


def kernel(
    ring,
    n_tp,
    token_ref,
    code_ref,
    share_ref,
    up_ref,
    out_ref,
    gain_ref,
    normed_ref,
    feats,
    staged,
    table,
    pair,
    code_middle,
    code_onward,
    code_packs,
    share_middle,
    share_onward,
    share_packs,
    codes,
    shares,
    tokens,
    row_vmem,
    row_smem,
    ups,
    outs,
    dots,
    dot_box,
    coefs,
    parts,
    inbox,
    inbox_x,
    inbox2,
    outbox,
    squares,
    load_sem,
    feat_sem,
    middle_sem,
    pack_sem,
    row_sem,
    dot_sem,
    sum_sem,
    square_sem,
    sent_sem,
):
    blocks = ring * ring
    held = up_ref.shape[0]
    half = feats.shape[1]
    toks = 2 * half
    cap = codes.shape[1]
    order = wave(ring)
    number = {uv: i for i, uv in enumerate(order)}
    me, mine = lax.axis_index("ep"), lax.axis_index("tp")
    z, y = me // ring, lax.rem(me, ring)
    turn = lambda k, by: lax.rem(k + by % ring, ring)
    column = lambda by: {"ep": turn(z, by) * ring + y}
    line = lambda by: {"ep": z * ring + turn(y, by)}
    across = lambda by: {"tp": lax.rem(mine + by, n_tp)}
    along = (column, line)

    def remote(src, dst, sent, landed, device):
        pltpu.make_async_remote_copy(
            src, dst, sent, landed, device_id=device, device_id_type=MESH
        ).start()

    own = number[0, 0]
    loads = [
        pltpu.make_async_copy(token_ref.at[pl.ds(h * half, half)], feats.at[h * blocks + own], load_sem.at[h])
        for h in range(2)
    ]
    tables = [
        pltpu.make_async_copy(ref, staged.at[i], load_sem.at[2 + i])
        for i, ref in enumerate((up_ref, out_ref))
    ]
    for load in loads + tables:
        load.start()
    barrier = pltpu.get_barrier_semaphore()
    peers = [f(by) for f in along for by in range(1, ring)] + [across(by) for by in range(1, n_tp)]
    for peer in peers:
        pl.semaphore_signal(barrier, inc=1, device_id=peer, device_id_type=MESH)
    for load in loads:
        load.wait()
    pl.semaphore_wait(barrier, len(peers))

    def place(h, q, p):
        return h * blocks + number[(q, p) if h == 0 else (p, q)]

    def pass_on(h, q, p):
        here = place(h, q, p)
        if (q, p) != (0, 0):
            arrived(feats.at[here], feat_sem.at[here])
        hops = [(h, way, place(h, (q + way) % ring, 0)) for way in beyond(ring, q, h == 0) if p == 0]
        hops += [(1 - h, way, place(h, q, (p + way) % ring)) for way in beyond(ring, p, q % 2 == 0)]
        for axis, way, there in hops:
            remote(feats.at[here], feats.at[there], sent_sem.at[0], feat_sem.at[there], along[axis](way))

    gathering = [functools.partial(pass_on, h, q, p) for q, p in reversed(order) for h in range(2)]

    parcels = (
        (code_ref, code_middle, code_onward, code_packs, codes),
        (share_ref, share_middle, share_onward, share_packs, shares),
    )

    def send_parcels():
        for kind, (parcel, middle, _, _, _) in enumerate(parcels):
            for by in range(1, ring):
                remote(parcel.at[turn(z, by)], middle.at[by], sent_sem.at[1 + kind], middle_sem.at[kind, by], column(by))
            middle[0] = parcel[z]

    def build_table():
        for load in tables:
            load.wait()
        for i in range(2):
            table[pl.ds(i, held, stride=2), :] = staged[i].astype(F32)

    def forward_parcels():
        for kind, (_, middle, onward, packs, _) in enumerate(parcels):
            for by in range(1, ring):
                arrived(middle.at[by], middle_sem.at[kind, by])
            for k in range(ring):
                for u in range(ring):
                    onward[k, u : u + 1, :] = middle[u, k : k + 1, :]
            for by in range(1, ring):
                remote(onward.at[turn(y, by)], packs.at[by], sent_sem.at[3 + kind], pack_sem.at[kind, by], line(by))
            packs[0] = onward[y]

    def open_packs():
        for kind, (_, _, _, packs, listed) in enumerate(parcels):
            for by in range(1, ring):
                arrived(packs.at[by], pack_sem.at[kind, by])
            for i, (u, v) in enumerate(order):
                listed[i : i + 1, :] = packs[v, u : u + 1, :]
        code = codes[...]
        row_vmem[...] = (code & (held - 1)) * 2
        tokens[...] = (code >> (held.bit_length() - 1)).astype(F32)

    def fetch_rows():
        copy = pltpu.make_async_copy(row_vmem, row_smem, row_sem)
        copy.start()
        copy.wait()

    def gather(start):
        def one(i, carry):
            for r in range(cap):
                pair[2 * r : 2 * r + 2, :] = table[pl.ds(row_smem[i, r], 2), :]
            ups[i] = pair[pl.ds(0, cap, stride=2), :].astype(BF16)
            outs[i] = pair[pl.ds(1, cap, stride=2), :].astype(BF16)
            return carry

        lax.fori_loop(start, start + GATHERS, one, 0)

    def interleave(first, second):
        done = 0
        for k, step in enumerate(first):
            step()
            upto = (k + 1) * len(second) // len(first)
            for step in second[done:upto]:
                step()
            done = upto

    early, middle_part, late = gathering[:2], gathering[2:34], gathering[34:]
    for step in early:
        step()
    send_parcels()
    for step in middle_part[:24]:
        step()
    forward_parcels()
    build_table()
    for step in middle_part[24:]:
        step()
    open_packs()
    for step in late[:4]:
        step()
    fetch_rows()
    interleave(late[4:], [functools.partial(gather, s) for s in range(0, blocks, GATHERS)])

    batch = blocks // BATCHES
    token = lax.broadcasted_iota(I32, (toks, cap), 0).astype(F32)

    def take_dots(b):
        def one(i, carry):
            feat = jnp.concatenate([feats[i], feats[blocks + i]], axis=0)
            every = lax.dot_general(feat, ups[i], CONTRACT_MINOR, preferred_element_type=F32)
            here = tokens[pl.ds(i, 1), :] == token
            dots[pl.ds(i, 1), :] = jnp.sum(jnp.where(here, every, 0.0), axis=0, keepdims=True)
            return carry

        lax.fori_loop(b * batch, (b + 1) * batch, one, 0)
        for by in range(1, n_tp):
            remote(
                dots.at[pl.ds(b * batch, batch)], dot_box.at[b, by], sent_sem.at[5 + b], dot_sem.at[b], across(by)
            )

    def take_coefs(b):
        arrived(dot_box.at[b, pl.ds(1, n_tp - 1)], dot_sem.at[b])
        which = slice(b * batch, (b + 1) * batch)
        total = dots[which, :]
        for by in range(1, n_tp):
            total = total + dot_box[b, by]
        coefs[which, :] = jax.nn.gelu(total) * shares[which, :]

    def mix(start):
        def one(i, carry):
            here = tokens[pl.ds(i, 1), :] == token
            coef = coefs[pl.ds(i, 1), :]
            coef_hi = coef.astype(BF16).astype(F32)
            spread = jnp.concatenate(
                [jnp.where(here, c, 0.0).astype(BF16) for c in (coef_hi, coef - coef_hi)], axis=1
            )
            both = jnp.concatenate([outs[i]] * 2, axis=0)
            parts[i] = jnp.dot(spread, both, preferred_element_type=F32)
            return carry

        lax.fori_loop(start, start + MIXES, one, 0)

    slots = {}

    def sem_of(*key):
        return sum_sem.at[slots.setdefault(key, len(slots))]

    def box(h, q, p, way):
        if p == 0 and way < 0:
            return inbox_x.at[h, q], sem_of("x", h, q)
        return inbox.at[place(h, q, p)], sem_of("i", h, q, p)

    def box2(h, q, way):
        if q == 0 and way < 0:
            return inbox2.at[h, ring], sem_of("x2", h)
        return inbox2.at[h, q], sem_of("i2", h, q)

    mixed = [None, None]

    def add_up(h, q, p):
        here = place(h, q, p)
        value = parts[here - h * blocks, h * half : (h + 1) * half]
        plus = q % 2 == 0
        came = [box(h, q, p, way) for way in beyond(ring, p, plus)]
        if p == 0:
            came += [box2(h, q, way) for way in beyond(ring, q, h == 0)]
        for ref, sem in came:
            arrived(ref, sem)
            value = value + ref[...].astype(F32)
        if (q, p) == (0, 0):
            mixed[h] = value
            return
        outbox[here] = value.astype(BF16)
        if p:
            way = heading(ring, p, plus)
            (ref, sem), axis = box(h, q, (p - way) % ring, way), 1 - h
        else:
            way = heading(ring, q, h == 0)
            (ref, sem), axis = box2(h, (q - way) % ring, way), h
        remote(outbox.at[here], ref, sent_sem.at[5 + BATCHES], sem, along[axis](-way))

    for b in range(BATCHES):
        take_dots(b)
    for b in range(BATCHES):
        take_coefs(b)
        for s in range(b * batch, (b + 1) * batch, MIXES):
            mix(s)
            for i in range(s, s + MIXES):
                for h in range(2):
                    add_up(h, *order[i][:: 1 - 2 * h])

    ones = jnp.ones((8, 2 * normed_ref.shape[1]), BF16)
    sums = []
    for h in range(2):
        square = mixed[h] * mixed[h]
        square_hi = square.astype(BF16).astype(F32)
        split = jnp.concatenate([square_hi.astype(BF16), (square - square_hi).astype(BF16)], axis=1)
        sums.append(lax.dot_general(ones, split, CONTRACT_MINOR, preferred_element_type=F32))
    which = lax.broadcasted_iota(I32, sums[0].shape, 0)
    squares[0] = jnp.where(which == 0, sums[0], sums[1])[:2]
    for by in range(1, n_tp):
        remote(squares.at[0], squares.at[by], sent_sem.at[6 + BATCHES], square_sem, across(by))
    arrived(squares.at[pl.ds(1, n_tp - 1)], square_sem)
    total = squares[0]
    for by in range(1, n_tp):
        total = total + squares[by]
    scale = lax.rsqrt(total / (normed_ref.shape[1] * n_tp) + 1e-06)
    same = lax.broadcasted_iota(I32, (half, half), 0) == lax.broadcasted_iota(I32, (half, half), 1)
    for h in range(2):
        scales = jnp.sum(jnp.where(same, scale[h : h + 1, :], 0.0), axis=1, keepdims=True)
        normed_ref[h * half : (h + 1) * half, :] = (mixed[h] * scales * gain_ref[...]).astype(BF16)

    arrived(feats.at[pl.ds(0, 2 * (blocks - 1))], sent_sem.at[0])
    for kind, (_, middle, _, packs, _) in enumerate(parcels):
        arrived(middle.at[pl.ds(1, ring - 1)], sent_sem.at[1 + kind])
        arrived(packs.at[pl.ds(1, ring - 1)], sent_sem.at[3 + kind])
    for b in range(BATCHES):
        arrived(dot_box.at[b, pl.ds(1, n_tp - 1)], sent_sem.at[5 + b])
    arrived(outbox.at[pl.ds(0, 2 * (blocks - 1))], sent_sem.at[5 + BATCHES])
    arrived(squares.at[pl.ds(1, n_tp - 1)], sent_sem.at[6 + BATCHES])


def body(tokens, experts, weights, up_table, out_table, gain):
    n_ep, n_tp = lax.axis_size("ep"), lax.axis_size("tp")
    ring = round(n_ep**0.5)
    toks, width = tokens.shape
    slots = experts.shape[1]
    held = up_table.shape[0]
    cap = 2 * toks * slots // n_ep
    half = toks // 2
    batch = n_ep // BATCHES
    any_space, vmem = pl.BlockSpec(memory_space=pl.ANY), pl.BlockSpec(memory_space=pltpu.VMEM)
    dma = pltpu.SemaphoreType.DMA
    codes, shares = pl.pallas_call(
        functools.partial(bucket_kernel, held),
        out_shape=(
            jax.ShapeDtypeStruct((ring, ring, cap), I32),
            jax.ShapeDtypeStruct((ring, ring, cap), F32),
        ),
        name="bucket",
    )(experts.T, weights.T)
    return pl.pallas_call(
        functools.partial(kernel, ring, n_tp),
        out_shape=jax.ShapeDtypeStruct((toks, width), BF16),
        in_specs=[any_space, vmem, vmem, any_space, any_space, vmem],
        out_specs=vmem,
        scratch_shapes=[
            pltpu.VMEM((2 * n_ep, half, width), BF16),
            pltpu.VMEM((2, held, width), BF16),
            pltpu.VMEM((2 * held, width), F32),
            pltpu.VMEM((2 * cap, width), F32),
            pltpu.VMEM((ring, ring, cap), I32),
            pltpu.VMEM((ring, ring, cap), I32),
            pltpu.VMEM((ring, ring, cap), I32),
            pltpu.VMEM((ring, ring, cap), F32),
            pltpu.VMEM((ring, ring, cap), F32),
            pltpu.VMEM((ring, ring, cap), F32),
            pltpu.VMEM((n_ep, cap), I32),
            pltpu.VMEM((n_ep, cap), F32),
            pltpu.VMEM((n_ep, cap), F32),
            pltpu.VMEM((n_ep, cap), I32),
            pltpu.SMEM((n_ep, cap), I32),
            pltpu.VMEM((n_ep, cap, width), BF16),
            pltpu.VMEM((n_ep, cap, width), BF16),
            pltpu.VMEM((n_ep, cap), F32),
            pltpu.VMEM((BATCHES, n_tp, batch, cap), F32),
            pltpu.VMEM((n_ep, cap), F32),
            pltpu.VMEM((n_ep, toks, width), F32),
            pltpu.VMEM((2 * n_ep, half, width), BF16),
            pltpu.VMEM((2, ring, half, width), BF16),
            pltpu.VMEM((2, ring + 1, half, width), BF16),
            pltpu.VMEM((2 * n_ep, half, width), BF16),
            pltpu.VMEM((n_tp, 2, half), F32),
            dma((4,)),
            dma((2 * n_ep,)),
            dma((2, ring)),
            dma((2, ring)),
            dma,
            dma((BATCHES,)),
            dma((2 * n_ep,)),
            dma,
            dma((7 + BATCHES,)),
        ],
        compiler_params=pltpu.CompilerParams(
            collective_id=0, has_side_effects=True, vmem_limit_bytes=56 << 20
        ),
        name="retrieve",
    )(tokens, codes, shares, up_table, out_table, gain[None, :])


def solution(mesh):
    placed = (P("ep", "tp"), P("ep", None), P("ep", None), P("ep", "tp"), P("ep", "tp"), P("tp"))
    return jax.shard_map(body, mesh=mesh, in_specs=placed, out_specs=P("ep", "tp"), check_vma=False)
```

```python
import functools

import jax
import jax.numpy as jnp
from jax import lax
from jax.experimental import pallas as pl
from jax.experimental.pallas import tpu as pltpu
from jax.sharding import PartitionSpec as P

F32, BF16, I32 = jnp.float32, jnp.bfloat16, jnp.int32
CONTRACT_MINOR = (((1,), (1,)), ((), ()))
MESH = pl.DeviceIdType.MESH
scope = jax.named_scope
CHUNKS = 2
BATCHES = 8
GATHERS = 2
UNROLL = 4
SLACK = 0.6
LATER = 10.0


def distance(ring, step):
    return min(step, ring - step)


def heading(ring, step, plus):
    if step == 0:
        return 0
    if 2 * step == ring:
        return 1 if plus else -1
    return 1 if 2 * step < ring else -1


def beyond(ring, step, plus):
    out = []
    for way in (1, -1):
        after = (step + way) % ring
        if after and heading(ring, after, plus) == way and (step == 0 or heading(ring, step, plus) == way):
            out.append(way)
    return out


def wave(ring):
    every = [(u, v) for u in range(ring) for v in range(ring)]
    return sorted(every, key=lambda uv: (-distance(ring, uv[0]) - distance(ring, uv[1]), uv))


def schedule(steps, slack, late):
    users = {}
    for name, (_, needs, _) in steps.items():
        for need in needs:
            users.setdefault(need, []).append(name)
    rank = {}
    pending = [(name, False) for name in steps]
    while pending:
        name, ready = pending.pop()
        ways = [(user, 0.0) for user in users.get(name, [])]
        ways += [(user, t + under_way) for _, t, under_way, m in steps[name][2] for user in users.get(m, [])]
        if ready:
            rank[name] = steps[name][0] + max((wait + rank[user] for user, wait in ways), default=0.0)
        elif name not in rank:
            pending.append((name, True))
            pending += [(user, False) for user, _ in ways if user not in rank]
    waits = {name: len(needs) for name, (_, needs, _) in steps.items()}
    at = {name: 0.0 for name in steps}
    ready = [name for name in steps if not waits[name]]
    now, busy, order = 0.0, {}, []

    def tell(key, time):
        for user in users.get(key, []):
            at[user] = max(at[user], time)
            waits[user] -= 1
            if not waits[user]:
                ready.append(user)

    def start(name):
        return max([at[name]] + [busy.get(link, 0.0) - slack for link, _, _, _ in steps[name][2] if link])

    while ready:
        starts = {name: start(name) for name in ready}
        now = max(now, min(starts.values()))
        name = max((n for n in ready if starts[n] <= now + 1e-9), key=lambda n: rank[n] - late(n))
        ready.remove(name)
        order.append(name)
        now += steps[name][0]
        tell(name, now)
        for link, t, under_way, m in steps[name][2]:
            begin = max(now, busy.get(link, 0.0)) if link else now
            busy[link] = begin + t
            tell(m, begin + t + under_way)
    assert len(order) == len(steps)
    return order


def arrived(ref, sem):
    pltpu.make_async_copy(ref, ref, sem).wait()


def bucket_kernel(
    rows_held, expert_hbm, weight_hbm, token_hbm, code_ref, share_ref, token_ref, expert_ref, weight_ref, load_sem
):
    loads = [
        pltpu.make_async_copy(src, dst, load_sem.at[i])
        for i, (src, dst) in enumerate(((expert_hbm, expert_ref), (weight_hbm, weight_ref), (token_hbm, token_ref)))
    ]
    for load in loads:
        load.start()
    slots, toks = expert_ref.shape
    ring, _, cap = code_ref.shape
    owners = ring * ring
    shift = rows_held.bit_length() - 1
    owner_no = lax.broadcasted_iota(I32, (owners, toks), 0)
    rank_no = lax.broadcasted_iota(I32, (cap, toks), 0)
    token_no = lax.broadcasted_iota(I32, (1, toks), 1).astype(F32)
    first = lax.broadcasted_iota(I32, (toks, toks), 0)
    second = lax.broadcasted_iota(I32, (toks, toks), 1)
    earlier = jnp.where(first < second, 1.0, 0.0).astype(BF16)
    ones = jnp.ones((toks, toks), BF16)
    before = jnp.zeros((owners, toks), F32)
    found = jnp.zeros((5 * owners, cap), F32)
    for load in loads:
        load.wait()
    for k in range(slots):
        expert = expert_ref[k : k + 1, :]
        local = expert & (rows_held - 1)
        mine = (expert >> shift) == owner_no
        onehot = jnp.where(mine, 1.0, 0.0).astype(BF16)
        rank = before + jnp.dot(onehot, earlier, preferred_element_type=F32)
        before = before + jnp.dot(onehot, ones, preferred_element_type=F32)
        rank = jnp.sum(jnp.where(mine, rank, 0.0), axis=0, keepdims=True).astype(I32)
        place = jnp.where(rank == rank_no, 1.0, 0.0).astype(BF16)
        weight = weight_ref[k : k + 1, :]
        weight_hi = weight.astype(BF16).astype(F32)
        pieces = (
            (local >> 8).astype(F32),
            (local & 255).astype(F32),
            token_no,
            weight_hi,
            weight - weight_hi,
        )
        what = jnp.concatenate([jnp.where(mine, p, 0.0).astype(BF16) for p in pieces], axis=0)
        found = found + lax.dot_general(what, place, CONTRACT_MINOR, preferred_element_type=F32)
    part = [found[i * owners : (i + 1) * owners] for i in range(5)]
    code = part[2] * float(rows_held) + part[0] * 256.0 + part[1]
    weight = part[3] + part[4]
    for k in range(ring):
        code_ref[k] = code[k * ring : (k + 1) * ring].astype(I32)
        share_ref[k] = weight[k * ring : (k + 1) * ring]


def kernel(ring, *refs):
    messages = 2 * CHUNKS * ring * ring
    dma = pltpu.SemaphoreType.DMA
    pl.run_scoped(
        functools.partial(inside, ring, *refs),
        load_sem=dma((3,)),
        feat_sem=dma((messages,)),
        middle_sem=dma((2, ring)),
        pack_sem=dma((2, ring)),
        row_sem=dma,
        dot_sem=dma((CHUNKS * BATCHES,)),
        sum_sem=dma((messages,)),
        square_sem=dma((CHUNKS,)),
        sent_sem=dma((8,)),
    )


def inside(
    ring,
    n_tp,
    token_ref,
    code_ref,
    share_ref,
    up_ref,
    out_ref,
    gain_hbm,
    normed_ref,
    feats,
    gain_ref,
    staged,
    table,
    pair,
    code_middle,
    code_onward,
    code_packs,
    share_middle,
    share_onward,
    share_packs,
    codes,
    shares,
    tokens,
    row_vmem,
    row_smem,
    ups,
    outs,
    dots,
    dot_box,
    coefs,
    parts,
    inbox,
    inbox_x,
    inbox2,
    outbox,
    mixed,
    squares,
    *,
    load_sem,
    feat_sem,
    middle_sem,
    pack_sem,
    row_sem,
    dot_sem,
    sum_sem,
    square_sem,
    sent_sem,
):
    blocks = ring * ring
    held, width = up_ref.shape
    rows = feats.shape[1]
    span = 2 * rows
    cap = codes.shape[1]
    order = wave(ring)
    number = {uv: i for i, uv in enumerate(order)}
    me, mine = lax.axis_index("ep"), lax.axis_index("tp")
    z, y = me // ring, lax.rem(me, ring)
    turn = lambda k, by: lax.rem(k + by % ring, ring)
    column = lambda by: {"ep": turn(z, by) * ring + y}
    line = lambda by: {"ep": z * ring + turn(y, by)}
    across = lambda by: {"tp": lax.rem(mine + by, n_tp)}
    along = (column, line)
    place = lambda h, q, p: number[(q, p) if h == 0 else (p, q)]
    slot = lambda c, h, q, p: (c * 2 + h) * blocks + place(h, q, p)

    def remote(src, dst, sent, landed, device):
        pltpu.make_async_remote_copy(
            src, dst, sent, landed, device_id=device, device_id_type=MESH
        ).start()

    loads = [
        pltpu.make_async_copy(src, dst, load_sem.at[i])
        for i, (src, dst) in enumerate(
            ((up_ref, staged.at[0]), (out_ref, staged.at[1]), (gain_hbm, gain_ref))
        )
    ]
    for load in loads:
        load.start()
    barrier = pltpu.get_barrier_semaphore()
    peers = [f(by) for f in along for by in range(1, ring)] + [across(by) for by in range(1, n_tp)]
    for peer in peers:
        pl.semaphore_signal(barrier, inc=1, device_id=peer, device_id_type=MESH)

    steps, actions = {}, {}

    def step(name, time, needs, sends, action):
        steps[name] = (time, needs, sends)
        actions[name] = action

    wire = rows * width * 2 / 46.6e3
    hop = 2.0

    def pass_on(c, h, q, p):
        here = slot(c, h, q, p)
        hops = [(h, way, slot(c, h, (q + way) % ring, 0)) for way in beyond(ring, q, h == 0) if p == 0]
        hops += [(1 - h, way, slot(c, h, q, (p + way) % ring)) for way in beyond(ring, p, q % 2 == 0)]

        def action():
            if (q, p) == (0, 0):
                source = token_ref.at[pl.ds((c * 2 + h) * rows, rows)]
                feats[here] = source[...]
            else:
                source = feats.at[here]
                arrived(source, feat_sem.at[here])
            for axis, way, there in hops:
                remote(source, feats.at[there], sent_sem.at[0], feat_sem.at[there], along[axis](way))

        needs = [] if (q, p) == (0, 0) else [("feat", here)]
        sends = [((axis, way), wire, hop, ("feat", there)) for axis, way, there in hops]
        step(("pass", c, h, q, p), 0.02 + 0.01 * len(hops), needs, sends, action)

    for c in range(CHUNKS):
        for h in range(2):
            for q, p in order:
                pass_on(c, h, q, p)

    parcels = (
        (code_ref, code_middle, code_onward, code_packs, codes),
        (share_ref, share_middle, share_onward, share_packs, shares),
    )

    def send_parcels():
        for kind, (parcel, middle, _, _, _) in enumerate(parcels):
            for by in range(1, ring):
                remote(parcel.at[turn(z, by)], middle.at[by], sent_sem.at[1 + kind], middle_sem.at[kind, by], column(by))
            middle[0] = parcel[z]

    def forward_parcels():
        for kind, (_, middle, onward, packs, _) in enumerate(parcels):
            for by in range(1, ring):
                arrived(middle.at[by], middle_sem.at[kind, by])
            for k in range(ring):
                for u in range(ring):
                    onward[k, u : u + 1, :] = middle[u, k : k + 1, :]
            for by in range(1, ring):
                remote(onward.at[turn(y, by)], packs.at[by], sent_sem.at[3 + kind], pack_sem.at[kind, by], line(by))
            packs[0] = onward[y]

    def open_packs():
        for kind, (_, _, _, packs, listed) in enumerate(parcels):
            for by in range(1, ring):
                arrived(packs.at[by], pack_sem.at[kind, by])
            for i, (u, v) in enumerate(order):
                listed[i : i + 1, :] = packs[v, u : u + 1, :]
        code = codes[...]
        row_vmem[...] = (code & (held - 1)) * 2
        tokens[...] = (code >> (held.bit_length() - 1)).astype(F32)

    fetch = pltpu.make_async_copy(row_vmem, row_smem, row_sem)
    letters = lambda axis, what: [((axis, way), 0.7, 4.0, (what, way)) for way in (1, -1)]
    step("send_parcels", 0.05, [], letters(0, "middle"), send_parcels)
    step("forward_parcels", 0.1, [("middle", 1), ("middle", -1)], letters(1, "pack"), forward_parcels)
    step("open_packs", 0.08, [("pack", 1), ("pack", -1)], [(None, 0.0, 0.1, "listed")], open_packs)
    step("fetch_rows", 0.02, ["listed"], [(None, 0.0, 1.1, "fetched")], fetch.start)
    step("rows", 0.01, ["fetched"], [], fetch.wait)

    def build_table():
        for load in loads:
            load.wait()
        for i in range(2):
            table[pl.ds(i, held, stride=2), :] = staged[i].astype(F32)

    step("build_table", 0.3, [], [], build_table)

    def gather(start):
        def one(i, carry):
            for r in range(cap):
                pair[2 * r : 2 * r + 2, :] = table[pl.ds(row_smem[i, r], 2), :]
            ups[i] = pair[pl.ds(0, cap, stride=2), :].astype(BF16)
            outs[i] = pair[pl.ds(1, cap, stride=2), :].astype(BF16)
            return carry

        lax.fori_loop(start, start + GATHERS, one, 0)

    for i in range(0, blocks, GATHERS):
        step(("gather", i), 0.125 * GATHERS, ["rows", "build_table"], [], functools.partial(gather, i))

    batch = blocks // BATCHES
    sublane = lax.broadcasted_iota(I32, (8, cap), 0).astype(F32)
    token = lax.broadcasted_iota(I32, (span, cap), 0).astype(F32)

    def in_fours(b, one):
        def four(k, carry):
            for i in range(UNROLL):
                one(b * batch + k * UNROLL + i)
            return carry

        lax.fori_loop(0, batch // UNROLL, four, 0)

    def take_dots(c, b):
        def one(i):
            feat = jnp.concatenate([feats[(c * 2 + h) * blocks + i] for h in range(2)], axis=0)
            every = lax.dot_general(feat, ups[i], CONTRACT_MINOR, preferred_element_type=F32)
            here = tokens[pl.ds(i, 1), :] - (sublane + float(c * span))
            sums = [None] * 4
            for g in range(span // 8):
                term = jnp.where(here == float(8 * g), every[8 * g : 8 * g + 8, :], 0.0)
                sums[g % 4] = term if sums[g % 4] is None else sums[g % 4] + term
            total = (sums[0] + sums[1]) + (sums[2] + sums[3])
            dots[c, pl.ds(i, 1), :] = jnp.sum(total, axis=0, keepdims=True)

        in_fours(b, one)
        some = pl.ds(b * batch, batch)
        for by in range(1, n_tp):
            remote(
                dots.at[c, some], dot_box.at[c, by, some], sent_sem.at[5], dot_sem.at[c * BATCHES + b], across(by)
            )

    def take_coefs(c, b):
        low, high = b * batch, (b + 1) * batch
        arrived(dot_box.at[c, pl.ds(1, n_tp - 1), pl.ds(low, batch)], dot_sem.at[c * BATCHES + b])
        total = dots[c, low:high, :]
        for by in range(1, n_tp):
            total = total + dot_box[c, by, low:high]
        coefs[c, low:high, :] = jax.nn.gelu(total) * shares[low:high, :]

        def one(i):
            here = tokens[pl.ds(i, 1), :] - float(c * span) == token
            coef = coefs[c, pl.ds(i, 1), :]
            coef_hi = coef.astype(BF16).astype(F32)
            spread = jnp.concatenate(
                [jnp.where(here, x, 0.0).astype(BF16) for x in (coef_hi, coef - coef_hi)], axis=1
            )
            both = jnp.concatenate([outs[i]] * 2, axis=0)
            parts[c, i] = jnp.dot(spread, both, preferred_element_type=F32)

        in_fours(b, one)

    share = 1.5 / CHUNKS
    for c in range(CHUNKS):
        for b in range(BATCHES):
            mine_of = range(b * batch, (b + 1) * batch)
            needs = [("gather", i) for i in mine_of if i % GATHERS == 0]
            needs += [("pass", c, h, *order[i][:: 1 - 2 * h]) for i in mine_of for h in range(2)]
            sends = [(("x",), 0.175 * batch, 5.0, ("totals", c, b))]
            step(("dots", c, b), 0.1 + 0.055 * batch * share, needs, sends, functools.partial(take_dots, c, b))
            step(("mix", c, b), 0.05 + 0.055 * batch * share, [("totals", c, b)], [], functools.partial(take_coefs, c, b))

    numbers = {}

    def box(*key):
        sem = sum_sem.at[numbers.setdefault(key, len(numbers))]
        kind, c, h, q, p, way = key
        if kind == 1:
            if p == 0 and way < 0:
                return inbox_x.at[(c * 2 + h) * ring + q], sem
            return inbox.at[slot(c, h, q, p)], sem
        return inbox2.at[(c * 2 + h) * (ring + 1) + (ring if q == 0 and way < 0 else q)], sem

    def add_up(c, h, q, p):
        here = slot(c, h, q, p)
        plus = q % 2 == 0
        came = [(1, c, h, q, p, way if p == 0 else 0) for way in beyond(ring, p, plus)]
        if p == 0:
            came += [(2, c, h, q, 0, way if q == 0 else 0) for way in beyond(ring, q, h == 0)]
        if p:
            way, axis = heading(ring, p, plus), 1 - h
            after = (p - way) % ring
            target = (1, c, h, q, after, way if after == 0 else 0)
        elif q:
            way, axis = heading(ring, q, h == 0), h
            after = (q - way) % ring
            target = (2, c, h, after, 0, way if after == 0 else 0)
        else:
            target = None

        def action():
            value = parts[c, place(h, q, p), h * rows : (h + 1) * rows]
            for key in came:
                ref, sem = box(*key)
                arrived(ref, sem)
                value = value + ref[...].astype(F32)
            if target is None:
                mixed[c, h * rows : (h + 1) * rows] = value
                return
            outbox[here] = value.astype(BF16)
            ref, sem = box(*target)
            remote(outbox.at[here], ref, sent_sem.at[6], sem, along[axis](-way))

        needs = [("mix", c, place(h, q, p) // batch)] + [("sum", *key) for key in came]
        sends = [((axis, -way), wire, hop, ("sum", *target))] if target else []
        step(("add", c, h, q, p), 0.02 + 0.03 / CHUNKS, needs, sends, action)

    for c in range(CHUNKS):
        for h in range(2):
            for q, p in order:
                add_up(c, h, q, p)

    def send_squares(c):
        square = mixed[c] * mixed[c]
        square_hi = square.astype(BF16).astype(F32)
        split = jnp.concatenate([square_hi.astype(BF16), (square - square_hi).astype(BF16)], axis=1)
        ones = jnp.ones((8, 2 * width), BF16)
        sums = lax.dot_general(ones, split, CONTRACT_MINOR, preferred_element_type=F32)
        squares[c, 0] = sums[:1]
        for by in range(1, n_tp):
            remote(squares.at[c, 0], squares.at[c, by], sent_sem.at[7], square_sem.at[c], across(by))

    def finish(c):
        arrived(squares.at[c, pl.ds(1, n_tp - 1)], square_sem.at[c])
        total = squares[c, 0]
        for by in range(1, n_tp):
            total = total + squares[c, by]
        scale = lax.rsqrt(total / (width * n_tp) + 1e-06)
        same = lax.broadcasted_iota(I32, (span, span), 0) == lax.broadcasted_iota(I32, (span, span), 1)
        scales = jnp.sum(jnp.where(same, scale, 0.0), axis=1, keepdims=True)
        normed_ref[c * span : (c + 1) * span, :] = (mixed[c] * scales * gain_ref[...]).astype(BF16)

    for c in range(CHUNKS):
        needs = [("add", c, h, 0, 0) for h in range(2)]
        step(("square", c), 0.2, needs, [(("x",), 0.4, 5.0, ("squares", c))], functools.partial(send_squares, c))
        step(("norm", c), 0.3, [("squares", c)], [], functools.partial(finish, c))

    chunk_of = lambda name: name[1] if isinstance(name, tuple) and name[0] != "gather" else 0
    plan = schedule(steps, SLACK, lambda name: LATER * chunk_of(name))
    with scope("barrier"):
        pl.semaphore_wait(barrier, len(peers))
    for name in plan:
        with scope(name if isinstance(name, str) else "_".join(map(str, name))):
            actions[name]()

    with scope("drain"):
        sums = CHUNKS * 2 * (blocks - 1)
        arrived(feats.at[pl.ds(0, sums)], sent_sem.at[0])
        for kind, (_, middle, _, packs, _) in enumerate(parcels):
            arrived(middle.at[pl.ds(1, ring - 1)], sent_sem.at[1 + kind])
            arrived(packs.at[pl.ds(1, ring - 1)], sent_sem.at[3 + kind])
        arrived(dot_box.at[:, pl.ds(1, n_tp - 1)], sent_sem.at[5])
        arrived(outbox.at[pl.ds(0, sums)], sent_sem.at[6])
        arrived(squares.at[:, pl.ds(1, n_tp - 1)], sent_sem.at[7])


def body(tokens, experts, weights, up_table, out_table, gain):
    n_ep, n_tp = lax.axis_size("ep"), lax.axis_size("tp")
    ring = round(n_ep**0.5)
    toks, width = tokens.shape
    slots = experts.shape[1]
    held = up_table.shape[0]
    cap = 2 * toks * slots // n_ep
    rows = toks // (2 * CHUNKS)
    blocks = 2 * CHUNKS * n_ep
    hbm, vmem = pl.BlockSpec(memory_space=pltpu.HBM), pl.BlockSpec(memory_space=pltpu.VMEM)
    in_hbm = lambda x: pltpu.with_memory_space_constraint(x, pltpu.HBM)
    codes, shares, near_tokens = pl.pallas_call(
        functools.partial(bucket_kernel, held),
        out_shape=(
            jax.ShapeDtypeStruct((ring, ring, cap), I32),
            jax.ShapeDtypeStruct((ring, ring, cap), F32),
            jax.ShapeDtypeStruct((toks, width), BF16),
        ),
        in_specs=[hbm] * 3,
        out_specs=(vmem, vmem, vmem),
        scratch_shapes=[
            pltpu.VMEM((slots, toks), I32),
            pltpu.VMEM((slots, toks), F32),
            pltpu.SemaphoreType.DMA((3,)),
        ],
        compiler_params=pltpu.CompilerParams(vmem_limit_bytes=4 << 20),
        name="bucket",
    )(in_hbm(experts.T), in_hbm(weights.T), in_hbm(tokens))
    return pl.pallas_call(
        functools.partial(kernel, ring, n_tp),
        out_shape=jax.ShapeDtypeStruct((toks, width), BF16),
        in_specs=[vmem, vmem, vmem, hbm, hbm, hbm],
        out_specs=vmem,
        scratch_shapes=[
            pltpu.VMEM((blocks, rows, width), BF16),
            pltpu.VMEM((1, width), F32),
            pltpu.VMEM((2, held, width), BF16),
            pltpu.VMEM((2 * held, width), F32),
            pltpu.VMEM((2 * cap, width), F32),
            pltpu.VMEM((ring, ring, cap), I32),
            pltpu.VMEM((ring, ring, cap), I32),
            pltpu.VMEM((ring, ring, cap), I32),
            pltpu.VMEM((ring, ring, cap), F32),
            pltpu.VMEM((ring, ring, cap), F32),
            pltpu.VMEM((ring, ring, cap), F32),
            pltpu.VMEM((n_ep, cap), I32),
            pltpu.VMEM((n_ep, cap), F32),
            pltpu.VMEM((n_ep, cap), F32),
            pltpu.VMEM((n_ep, cap), I32),
            pltpu.SMEM((n_ep, cap), I32),
            pltpu.VMEM((n_ep, cap, width), BF16),
            pltpu.VMEM((n_ep, cap, width), BF16),
            pltpu.VMEM((CHUNKS, n_ep, cap), F32),
            pltpu.VMEM((CHUNKS, n_tp, n_ep, cap), F32),
            pltpu.VMEM((CHUNKS, n_ep, cap), F32),
            pltpu.VMEM((CHUNKS, n_ep, 2 * rows, width), F32),
            pltpu.VMEM((blocks, rows, width), BF16),
            pltpu.VMEM((2 * CHUNKS * ring, rows, width), BF16),
            pltpu.VMEM((2 * CHUNKS * (ring + 1), rows, width), BF16),
            pltpu.VMEM((blocks, rows, width), BF16),
            pltpu.VMEM((CHUNKS, 2 * rows, width), F32),
            pltpu.VMEM((CHUNKS, n_tp, 1, 2 * rows), F32),
        ],
        compiler_params=pltpu.CompilerParams(
            collective_id=0, has_side_effects=True, vmem_limit_bytes=44 << 20
        ),
        name="retrieve",
    )(near_tokens, codes, shares, in_hbm(up_table), in_hbm(out_table), in_hbm(gain[None, :]))


def solution(mesh):
    placed = (P("ep", "tp"), P("ep", None), P("ep", None), P("ep", "tp"), P("ep", "tp"), P("tp"))
    return jax.shard_map(body, mesh=mesh, in_specs=placed, out_specs=P("ep", "tp"), check_vma=False)
```

```python
import functools

import jax
import jax.numpy as jnp
from jax import lax
from jax.experimental import pallas as pl
from jax.experimental.pallas import tpu as pltpu
from jax.sharding import PartitionSpec as P

F32, BF16, I32 = jnp.float32, jnp.bfloat16, jnp.int32
CONTRACT_MINOR = (((1,), (1,)), ((), ()))
MESH = pl.DeviceIdType.MESH
scope = jax.named_scope
HOP = {(0, 1): 2.2, (0, -1): 2.4, (1, 1): 2.4, (1, -1): 2.4}
WIRE, SLACK, ACROSS, LETTER, PICK = 0.36, 0.4, 6, 5, 0.165
SOONER = {
    ("pass", 0): 11, ("pass", 1): 2, ("dots", 0): -12, ("dots", 1): -14, ("mix", 0): 19,
    ("mix", 1): 2, ("add", 0): 14, ("add", 1): -5, ("gather", 0): 7,
}
NEXT_BATCH = 6
CHUNKS = 2
BATCHES = 8
GATHERS = 2


def distance(ring, step):
    return min(step, ring - step)


def heading(ring, step, plus):
    if step == 0:
        return 0
    if 2 * step == ring:
        return 1 if plus else -1
    return 1 if 2 * step < ring else -1


def beyond(ring, step, plus):
    out = []
    for way in (1, -1):
        after = (step + way) % ring
        if after and heading(ring, after, plus) == way and (step == 0 or heading(ring, step, plus) == way):
            out.append(way)
    return out


def far_first(ring):
    return sorted(range(1, ring), key=lambda by: -distance(ring, by))


def wave(ring):
    every = [(u, v) for u in range(ring) for v in range(ring)]
    return sorted(every, key=lambda uv: (-distance(ring, uv[0]) - distance(ring, uv[1]), uv))


def schedule(steps, slack, late):
    users = {}
    for name, (_, needs, _) in steps.items():
        for need in needs:
            users.setdefault(need, []).append(name)
    rank = {}
    pending = [(name, False) for name in steps]
    while pending:
        name, ready = pending.pop()
        ways = [(user, 0.0) for user in users.get(name, [])]
        ways += [(user, t + under_way) for _, t, under_way, m in steps[name][2] for user in users.get(m, [])]
        if ready:
            rank[name] = steps[name][0] + max((wait + rank[user] for user, wait in ways), default=0.0)
        elif name not in rank:
            pending.append((name, True))
            pending += [(user, False) for user, _ in ways if user not in rank]
    waits = {name: len(needs) for name, (_, needs, _) in steps.items()}
    at = {name: 0.0 for name in steps}
    ready = [name for name in steps if not waits[name]]
    now, busy, order = 0.0, {}, []

    def tell(key, time):
        for user in users.get(key, []):
            at[user] = max(at[user], time)
            waits[user] -= 1
            if not waits[user]:
                ready.append(user)

    def start(name):
        return max([at[name]] + [busy.get(link, 0.0) - slack for link, _, _, _ in steps[name][2] if link])

    while ready:
        starts = {name: start(name) for name in ready}
        now = max(now, min(starts.values()))
        name = max((n for n in ready if starts[n] <= now + 1e-9), key=lambda n: rank[n] - late(n))
        ready.remove(name)
        order.append(name)
        now += steps[name][0]
        tell(name, now)
        for link, t, under_way, m in steps[name][2]:
            begin = max(now, busy.get(link, 0.0)) if link else now
            busy[link] = begin + t
            tell(m, begin + t + under_way)
    assert len(order) == len(steps)
    return order


def arrived(ref, sem):
    pltpu.make_async_copy(ref, ref, sem).wait()


def bucket_kernel(
    rows_held, expert_hbm, weight_hbm, token_hbm, code_ref, share_ref, token_ref, expert_ref, weight_ref, load_sem
):
    loads = [
        pltpu.make_async_copy(src, dst, load_sem.at[i])
        for i, (src, dst) in enumerate(((expert_hbm, expert_ref), (weight_hbm, weight_ref), (token_hbm, token_ref)))
    ]
    for load in loads:
        load.start()
    slots, toks = expert_ref.shape
    ring, _, cap = code_ref.shape
    owners = ring * ring
    shift = rows_held.bit_length() - 1
    owner_no = lax.broadcasted_iota(I32, (owners, toks), 0)
    rank_no = lax.broadcasted_iota(I32, (cap, toks), 0)
    token_no = lax.broadcasted_iota(I32, (1, toks), 1).astype(F32)
    first = lax.broadcasted_iota(I32, (toks, toks), 0)
    second = lax.broadcasted_iota(I32, (toks, toks), 1)
    earlier = jnp.where(first < second, 1.0, 0.0).astype(BF16)
    ones = jnp.ones((toks, 128), BF16)
    for load in loads:
        load.wait()
    experts = [expert_ref[k : k + 1, :] for k in range(slots)]
    mine = [(expert >> shift) == owner_no for expert in experts]
    onehot = jnp.concatenate([jnp.where(m, 1.0, 0.0).astype(BF16) for m in mine], axis=0)
    ahead = jnp.dot(onehot, earlier, preferred_element_type=F32)
    total = jnp.dot(onehot, ones, preferred_element_type=F32)
    before = jnp.zeros((owners, ones.shape[1]), F32)
    what, where = [], []
    for k in range(slots):
        rows = slice(k * owners, (k + 1) * owners)
        rank = ahead[rows] + jnp.concatenate([before] * (toks // ones.shape[1]), axis=1)
        before = before + total[rows]
        rank = jnp.sum(jnp.where(mine[k], rank, 0.0), axis=0, keepdims=True).astype(I32)
        where.append(jnp.where(rank == rank_no, 1.0, 0.0).astype(BF16))
        local = experts[k] & (rows_held - 1)
        weight = weight_ref[k : k + 1, :]
        weight_hi = weight.astype(BF16).astype(F32)
        pieces = (
            (local >> 8).astype(F32),
            (local & 255).astype(F32),
            token_no,
            weight_hi,
            weight - weight_hi,
        )
        what.append(jnp.concatenate([jnp.where(mine[k], p, 0.0).astype(BF16) for p in pieces], axis=0))
    found = lax.dot_general(
        jnp.concatenate(what, axis=1), jnp.concatenate(where, axis=1), CONTRACT_MINOR, preferred_element_type=F32
    )
    part = [found[i * owners : (i + 1) * owners] for i in range(5)]
    code = part[2] * float(rows_held) + part[0] * 256.0 + part[1]
    weight = part[3] + part[4]
    for k in range(ring):
        code_ref[k] = code[k * ring : (k + 1) * ring].astype(I32)
        share_ref[k] = weight[k * ring : (k + 1) * ring]


def kernel(ring, *refs):
    messages = 2 * CHUNKS * ring * ring
    dma = pltpu.SemaphoreType.DMA
    pl.run_scoped(
        functools.partial(inside, ring, *refs),
        load_sem=dma((3,)),
        feat_sem=dma((messages,)),
        middle_sem=dma((2, ring)),
        pack_sem=dma((2, ring)),
        row_sem=dma,
        dot_sem=dma((CHUNKS * BATCHES,)),
        sum_sem=dma((messages,)),
        square_sem=dma((CHUNKS,)),
        sent_sem=dma((8,)),
    )


def inside(
    ring,
    n_tp,
    token_ref,
    code_ref,
    share_ref,
    up_ref,
    out_ref,
    gain_hbm,
    normed_ref,
    feats,
    gain_ref,
    staged,
    table,
    pair,
    code_middle,
    code_onward,
    code_packs,
    share_middle,
    share_onward,
    share_packs,
    codes,
    shares,
    tokens,
    row_vmem,
    row_smem,
    ups,
    outs,
    dots,
    dot_box,
    coefs,
    parts,
    inbox,
    inbox_x,
    inbox2,
    outbox,
    mixed,
    squares,
    *,
    load_sem,
    feat_sem,
    middle_sem,
    pack_sem,
    row_sem,
    dot_sem,
    sum_sem,
    square_sem,
    sent_sem,
):
    blocks = ring * ring
    held, width = up_ref.shape
    rows = feats.shape[1]
    span = 2 * rows
    cap = codes.shape[1]
    order = wave(ring)
    number = {uv: i for i, uv in enumerate(order)}
    me, mine = lax.axis_index("ep"), lax.axis_index("tp")
    z, y = me // ring, lax.rem(me, ring)
    turn = lambda k, by: lax.rem(k + by % ring, ring)
    column = lambda by: {"ep": turn(z, by) * ring + y}
    line = lambda by: {"ep": z * ring + turn(y, by)}
    across = lambda by: {"tp": lax.rem(mine + by, n_tp)}
    along = (column, line)
    place = lambda h, q, p: number[(q, p) if h == 0 else (p, q)]
    slot = lambda c, h, q, p: (c * 2 + h) * blocks + place(h, q, p)

    def remote(src, dst, sent, landed, device):
        pltpu.make_async_remote_copy(
            src, dst, sent, landed, device_id=device, device_id_type=MESH
        ).start()

    loads = [
        pltpu.make_async_copy(src, dst, load_sem.at[i])
        for i, (src, dst) in enumerate(
            ((up_ref, staged.at[0]), (out_ref, staged.at[1]), (gain_hbm, gain_ref))
        )
    ]
    for load in loads:
        load.start()
    barrier = pltpu.get_barrier_semaphore()
    peers = [f(by) for f in along for by in range(1, ring)] + [across(by) for by in range(1, n_tp)]
    for peer in peers:
        pl.semaphore_signal(barrier, inc=1, device_id=peer, device_id_type=MESH)

    steps, actions = {}, {}

    def step(name, time, needs, sends, action):
        steps[name] = (time, needs, sends)
        actions[name] = action

    wire = WIRE * 2 / CHUNKS

    def pass_on(c, h, q, p):
        here = slot(c, h, q, p)
        hops = [(h, way, slot(c, h, (q + way) % ring, 0)) for way in beyond(ring, q, h == 0) if p == 0]
        hops += [(1 - h, way, slot(c, h, q, (p + way) % ring)) for way in beyond(ring, p, q % 2 == 0)]

        def action():
            if (q, p) == (0, 0):
                source = token_ref.at[pl.ds((c * 2 + h) * rows, rows)]
                feats[here] = source[...]
            else:
                source = feats.at[here]
                arrived(source, feat_sem.at[here])
            for axis, way, there in hops:
                remote(source, feats.at[there], sent_sem.at[0], feat_sem.at[there], along[axis](way))

        needs = [] if (q, p) == (0, 0) else [("feat", here)]
        sends = [((axis, way), wire, HOP[axis, way], ("feat", there)) for axis, way, there in hops]
        step(("pass", c, h, q, p), 0.02, needs, sends, action)

    for c in range(CHUNKS):
        for h in range(2):
            for q, p in order:
                pass_on(c, h, q, p)

    parcels = (
        (code_ref, code_middle, code_onward, code_packs, codes),
        (share_ref, share_middle, share_onward, share_packs, shares),
    )

    def send_parcels():
        for kind, (parcel, middle, _, _, _) in enumerate(parcels):
            for by in far_first(ring):
                remote(parcel.at[turn(z, by)], middle.at[by], sent_sem.at[1 + kind], middle_sem.at[kind, by], column(by))
            middle[0] = parcel[z]

    def forward_parcels():
        for kind, (_, middle, onward, packs, _) in enumerate(parcels):
            for by in range(1, ring):
                arrived(middle.at[by], middle_sem.at[kind, by])
            for k in range(ring):
                for u in range(ring):
                    onward[k, u : u + 1, :] = middle[u, k : k + 1, :]
            for by in far_first(ring):
                remote(onward.at[turn(y, by)], packs.at[by], sent_sem.at[3 + kind], pack_sem.at[kind, by], line(by))
            packs[0] = onward[y]

    def open_packs():
        for kind, (_, _, _, packs, listed) in enumerate(parcels):
            for by in range(1, ring):
                arrived(packs.at[by], pack_sem.at[kind, by])
            for i, (u, v) in enumerate(order):
                listed[i : i + 1, :] = packs[v, u : u + 1, :]
        code = codes[...]
        row_vmem[...] = (code & (held - 1)) * 2
        tokens[...] = (code >> (held.bit_length() - 1)).astype(F32)

    fetch = pltpu.make_async_copy(row_vmem, row_smem, row_sem)
    letters = lambda axis, what: [((axis, way), 0.7, LETTER, (what, way)) for way in (1, -1)]
    step("send_parcels", 0.05, [], letters(0, "middle"), send_parcels)
    step("forward_parcels", 0.1, [("middle", 1), ("middle", -1)], letters(1, "pack"), forward_parcels)
    step("open_packs", 0.08, [("pack", 1), ("pack", -1)], [(None, 0.0, 0.1, "listed")], open_packs)
    step("fetch_rows", 0.02, ["listed"], [(None, 0.0, 1.1, "fetched")], fetch.start)
    step("rows", 0.01, ["fetched"], [], fetch.wait)

    def build_table():
        for load in loads:
            load.wait()
        for i in range(2):
            table[pl.ds(i, held, stride=2), :] = staged[i].astype(F32)

    step("build_table", 0.3, [], [], build_table)

    def gather(start):
        for i in range(start, start + GATHERS):
            both = pair.at[i % 2]
            for r in range(cap):
                both[2 * r : 2 * r + 2, :] = table[pl.ds(row_smem[i, r], 2), :]
            ups[i] = both[pl.ds(0, cap, stride=2), :].astype(BF16)
            outs[i] = both[pl.ds(1, cap, stride=2), :].astype(BF16)

    for i in range(0, blocks, GATHERS):
        step(("gather", i), PICK, ["rows", "build_table"], [], functools.partial(gather, i))

    batch = blocks // BATCHES
    sublane = lax.broadcasted_iota(I32, (8, cap), 0).astype(F32)
    token = lax.broadcasted_iota(I32, (span, cap), 0).astype(F32)

    def take_dots(c, b):
        def one(i):
            feat = jnp.concatenate([feats[(c * 2 + h) * blocks + i] for h in range(2)], axis=0)
            every = lax.dot_general(feat, ups[i], CONTRACT_MINOR, preferred_element_type=F32)
            here = tokens[i : i + 1, :] - (sublane + float(c * span))
            sums = [None] * 4
            for g in range(span // 8):
                term = jnp.where(here == float(8 * g), every[8 * g : 8 * g + 8, :], 0.0)
                sums[g % 4] = term if sums[g % 4] is None else sums[g % 4] + term
            total = (sums[0] + sums[1]) + (sums[2] + sums[3])
            dots[c, i : i + 1, :] = jnp.sum(total, axis=0, keepdims=True)

        for i in range(b * batch, (b + 1) * batch):
            one(i)
        some = pl.ds(b * batch, batch)
        for by in far_first(n_tp):
            remote(
                dots.at[c, some], dot_box.at[c, by, some], sent_sem.at[5], dot_sem.at[c * BATCHES + b], across(by)
            )

    def take_coefs(c, b):
        low, high = b * batch, (b + 1) * batch
        arrived(dot_box.at[c, pl.ds(1, n_tp - 1), pl.ds(low, batch)], dot_sem.at[c * BATCHES + b])
        total = dots[c, low:high, :]
        for by in range(1, n_tp):
            total = total + dot_box[c, by, low:high]
        coefs[c, low:high, :] = jax.nn.gelu(total) * shares[low:high, :]

        def one(i):
            here = tokens[i : i + 1, :] - float(c * span) == token
            coef = coefs[c, i : i + 1, :]
            coef_hi = coef.astype(BF16).astype(F32)
            spread = jnp.concatenate(
                [jnp.where(here, x, 0.0).astype(BF16) for x in (coef_hi, coef - coef_hi)], axis=1
            )
            both = jnp.concatenate([outs[i]] * 2, axis=0)
            parts[c, i] = jnp.dot(spread, both, preferred_element_type=F32)

        for i in range(b * batch, (b + 1) * batch):
            one(i)

    each = 0.66 / CHUNKS
    for c in range(CHUNKS):
        for b in range(BATCHES):
            mine_of = range(b * batch, (b + 1) * batch)
            needs = [("gather", i) for i in mine_of if i % GATHERS == 0]
            needs += [("pass", c, h, *order[i][:: 1 - 2 * h]) for i in mine_of for h in range(2)]
            sends = [(("x",), 0.175 * batch, ACROSS, ("totals", c, b))]
            step(("dots", c, b), each, needs, sends, functools.partial(take_dots, c, b))
            step(("mix", c, b), each, [("totals", c, b)], [], functools.partial(take_coefs, c, b))

    numbers = {}

    def box(*key):
        sem = sum_sem.at[numbers.setdefault(key, len(numbers))]
        kind, c, h, q, p, way = key
        if kind == 1:
            if p == 0 and way < 0:
                return inbox_x.at[(c * 2 + h) * ring + q], sem
            return inbox.at[slot(c, h, q, p)], sem
        return inbox2.at[(c * 2 + h) * (ring + 1) + (ring if q == 0 and way < 0 else q)], sem

    def add_up(c, h, q, p):
        here = slot(c, h, q, p)
        plus = q % 2 == 0
        came = [(1, c, h, q, p, way if p == 0 else 0) for way in beyond(ring, p, plus)]
        if p == 0:
            came += [(2, c, h, q, 0, way if q == 0 else 0) for way in beyond(ring, q, h == 0)]
        if p:
            way, axis = heading(ring, p, plus), 1 - h
            after = (p - way) % ring
            target = (1, c, h, q, after, way if after == 0 else 0)
        elif q:
            way, axis = heading(ring, q, h == 0), h
            after = (q - way) % ring
            target = (2, c, h, after, 0, way if after == 0 else 0)
        else:
            target = None

        def action():
            value = parts[c, place(h, q, p), h * rows : (h + 1) * rows]
            for key in came:
                ref, sem = box(*key)
                arrived(ref, sem)
                value = value + ref[...].astype(F32)
            if target is None:
                mixed[c, h * rows : (h + 1) * rows] = value
                return
            outbox[here] = value.astype(BF16)
            ref, sem = box(*target)
            remote(outbox.at[here], ref, sent_sem.at[6], sem, along[axis](-way))

        needs = [("mix", c, place(h, q, p) // batch)] + [("sum", *key) for key in came]
        sends = [((axis, -way), wire, HOP[axis, -way], ("sum", *target))] if target else []
        step(("add", c, h, q, p), 0.045, needs, sends, action)

    for c in range(CHUNKS):
        for h in range(2):
            for q, p in order:
                add_up(c, h, q, p)

    def send_squares(c):
        square = mixed[c] * mixed[c]
        square_hi = square.astype(BF16).astype(F32)
        split = jnp.concatenate([square_hi.astype(BF16), (square - square_hi).astype(BF16)], axis=1)
        ones = jnp.ones((8, 2 * width), BF16)
        sums = lax.dot_general(ones, split, CONTRACT_MINOR, preferred_element_type=F32)
        squares[c, 0] = sums[:1]
        for by in far_first(n_tp):
            remote(squares.at[c, 0], squares.at[c, by], sent_sem.at[7], square_sem.at[c], across(by))

    def finish(c):
        arrived(squares.at[c, pl.ds(1, n_tp - 1)], square_sem.at[c])
        total = squares[c, 0]
        for by in range(1, n_tp):
            total = total + squares[c, by]
        scale = lax.rsqrt(total / (width * n_tp) + 1e-06)
        same = lax.broadcasted_iota(I32, (span, span), 0) == lax.broadcasted_iota(I32, (span, span), 1)
        scales = jnp.sum(jnp.where(same, scale, 0.0), axis=1, keepdims=True)
        normed_ref[c * span : (c + 1) * span, :] = (mixed[c] * scales * gain_ref[...]).astype(BF16)

    for c in range(CHUNKS):
        needs = [("add", c, h, 0, 0) for h in range(2)]
        step(("square", c), 0.2, needs, [(("x",), 0.4, ACROSS, ("squares", c))], functools.partial(send_squares, c))
        step(("norm", c), 0.3, [("squares", c)], [], functools.partial(finish, c))

    def late(name):
        if isinstance(name, str):
            return -5
        kind, k = name[:2]
        if kind in ("square", "norm"):
            return -20
        wait = -SOONER[kind, 0 if kind == "gather" else k]
        if kind == "gather":
            return wait + NEXT_BATCH * (k // batch)
        return wait + NEXT_BATCH * name[2] * 0.5 if kind in ("dots", "mix") else wait

    plan = schedule(steps, SLACK, late)
    with scope("barrier"):
        pl.semaphore_wait(barrier, len(peers))
    for name in plan:
        with scope(name if isinstance(name, str) else "_".join(map(str, name))):
            actions[name]()

    with scope("drain"):
        sums = CHUNKS * 2 * (blocks - 1)
        arrived(feats.at[pl.ds(0, sums)], sent_sem.at[0])
        for kind, (_, middle, _, packs, _) in enumerate(parcels):
            arrived(middle.at[pl.ds(1, ring - 1)], sent_sem.at[1 + kind])
            arrived(packs.at[pl.ds(1, ring - 1)], sent_sem.at[3 + kind])
        arrived(dot_box.at[:, pl.ds(1, n_tp - 1)], sent_sem.at[5])
        arrived(outbox.at[pl.ds(0, sums)], sent_sem.at[6])
        arrived(squares.at[:, pl.ds(1, n_tp - 1)], sent_sem.at[7])


def body(tokens, experts, weights, up_table, out_table, gain):
    n_ep, n_tp = lax.axis_size("ep"), lax.axis_size("tp")
    ring = round(n_ep**0.5)
    toks, width = tokens.shape
    slots = experts.shape[1]
    held = up_table.shape[0]
    cap = 2 * toks * slots // n_ep
    rows = toks // (2 * CHUNKS)
    blocks = 2 * CHUNKS * n_ep
    hbm, vmem = pl.BlockSpec(memory_space=pltpu.HBM), pl.BlockSpec(memory_space=pltpu.VMEM)
    in_hbm = lambda x: pltpu.with_memory_space_constraint(x, pltpu.HBM)
    codes, shares, near_tokens = pl.pallas_call(
        functools.partial(bucket_kernel, held),
        out_shape=(
            jax.ShapeDtypeStruct((ring, ring, cap), I32),
            jax.ShapeDtypeStruct((ring, ring, cap), F32),
            jax.ShapeDtypeStruct((toks, width), BF16),
        ),
        in_specs=[hbm] * 3,
        out_specs=(vmem, vmem, vmem),
        scratch_shapes=[
            pltpu.VMEM((slots, toks), I32),
            pltpu.VMEM((slots, toks), F32),
            pltpu.SemaphoreType.DMA((3,)),
        ],
        compiler_params=pltpu.CompilerParams(vmem_limit_bytes=4 << 20),
        name="bucket",
    )(in_hbm(experts.T), in_hbm(weights.T), in_hbm(tokens))
    return pl.pallas_call(
        functools.partial(kernel, ring, n_tp),
        out_shape=jax.ShapeDtypeStruct((toks, width), BF16),
        in_specs=[vmem, vmem, vmem, hbm, hbm, hbm],
        out_specs=vmem,
        scratch_shapes=[
            pltpu.VMEM((blocks, rows, width), BF16),
            pltpu.VMEM((1, width), F32),
            pltpu.VMEM((2, held, width), BF16),
            pltpu.VMEM((2 * held, width), F32),
            pltpu.VMEM((2, 2 * cap, width), F32),
            pltpu.VMEM((ring, ring, cap), I32),
            pltpu.VMEM((ring, ring, cap), I32),
            pltpu.VMEM((ring, ring, cap), I32),
            pltpu.VMEM((ring, ring, cap), F32),
            pltpu.VMEM((ring, ring, cap), F32),
            pltpu.VMEM((ring, ring, cap), F32),
            pltpu.VMEM((n_ep, cap), I32),
            pltpu.VMEM((n_ep, cap), F32),
            pltpu.VMEM((n_ep, cap), F32),
            pltpu.VMEM((n_ep, cap), I32),
            pltpu.SMEM((n_ep, cap), I32),
            pltpu.VMEM((n_ep, cap, width), BF16),
            pltpu.VMEM((n_ep, cap, width), BF16),
            pltpu.VMEM((CHUNKS, n_ep, cap), F32),
            pltpu.VMEM((CHUNKS, n_tp, n_ep, cap), F32),
            pltpu.VMEM((CHUNKS, n_ep, cap), F32),
            pltpu.VMEM((CHUNKS, n_ep, 2 * rows, width), F32),
            pltpu.VMEM((blocks, rows, width), BF16),
            pltpu.VMEM((2 * CHUNKS * ring, rows, width), BF16),
            pltpu.VMEM((2 * CHUNKS * (ring + 1), rows, width), BF16),
            pltpu.VMEM((blocks, rows, width), BF16),
            pltpu.VMEM((CHUNKS, 2 * rows, width), F32),
            pltpu.VMEM((CHUNKS, n_tp, 1, 2 * rows), F32),
        ],
        compiler_params=pltpu.CompilerParams(
            collective_id=0, has_side_effects=True, vmem_limit_bytes=44 << 20
        ),
        name="retrieve",
    )(near_tokens, codes, shares, in_hbm(up_table), in_hbm(out_table), in_hbm(gain[None, :]))


def solution(mesh):
    placed = (P("ep", "tp"), P("ep", None), P("ep", None), P("ep", "tp"), P("ep", "tp"), P("tp"))
    return jax.shard_map(body, mesh=mesh, in_specs=placed, out_specs=P("ep", "tp"), check_vma=False)
```

```python
import functools

import jax
import jax.numpy as jnp
from jax import lax
from jax.experimental import pallas as pl
from jax.experimental.pallas import tpu as pltpu
from jax.sharding import PartitionSpec as P

F32, BF16, I32 = jnp.float32, jnp.bfloat16, jnp.int32
CONTRACT_MINOR = (((1,), (1,)), ((), ()))
MESH = pl.DeviceIdType.MESH
scope = jax.named_scope
HOP = {(0, 1): 2.2, (0, -1): 2.4, (1, 1): 2.4, (1, -1): 2.4}
WIRE, SLACK, ACROSS, LETTER, PICK = 0.36, 0.4, 6, 5, 0.165
SOONER = {
    ("pass", 0): 11, ("pass", 1): 2, ("dots", 0): -12, ("dots", 1): -14, ("mix", 0): 19,
    ("mix", 1): 2, ("add", 0): 14, ("add", 1): -5, ("gather", 0): 7,
}
NEXT_BATCH = 6
CHUNKS = 2
BATCHES = 8
GATHERS = 2


def distance(ring, step):
    return min(step, ring - step)


def heading(ring, step, plus):
    if step == 0:
        return 0
    if 2 * step == ring:
        return 1 if plus else -1
    return 1 if 2 * step < ring else -1


def beyond(ring, step, plus):
    out = []
    for way in (1, -1):
        after = (step + way) % ring
        if after and heading(ring, after, plus) == way and (step == 0 or heading(ring, step, plus) == way):
            out.append(way)
    return out


def far_first(ring):
    return sorted(range(1, ring), key=lambda by: -distance(ring, by))


def wave(ring):
    every = [(u, v) for u in range(ring) for v in range(ring)]
    return sorted(every, key=lambda uv: (-distance(ring, uv[0]) - distance(ring, uv[1]), uv))


def schedule(steps, slack, late):
    users = {}
    for name, (_, needs, _) in steps.items():
        for need in needs:
            users.setdefault(need, []).append(name)
    rank = {}
    pending = [(name, False) for name in steps]
    while pending:
        name, ready = pending.pop()
        ways = [(user, 0.0) for user in users.get(name, [])]
        ways += [(user, t + under_way) for _, t, under_way, m in steps[name][2] for user in users.get(m, [])]
        if ready:
            rank[name] = steps[name][0] + max((wait + rank[user] for user, wait in ways), default=0.0)
        elif name not in rank:
            pending.append((name, True))
            pending += [(user, False) for user, _ in ways if user not in rank]
    waits = {name: len(needs) for name, (_, needs, _) in steps.items()}
    at = {name: 0.0 for name in steps}
    ready = [name for name in steps if not waits[name]]
    now, busy, order = 0.0, {}, []

    def tell(key, time):
        for user in users.get(key, []):
            at[user] = max(at[user], time)
            waits[user] -= 1
            if not waits[user]:
                ready.append(user)

    def start(name):
        return max([at[name]] + [busy.get(link, 0.0) - slack for link, _, _, _ in steps[name][2] if link])

    while ready:
        starts = {name: start(name) for name in ready}
        now = max(now, min(starts.values()))
        name = max((n for n in ready if starts[n] <= now + 1e-9), key=lambda n: rank[n] - late(n))
        ready.remove(name)
        order.append(name)
        now += steps[name][0]
        tell(name, now)
        for link, t, under_way, m in steps[name][2]:
            begin = max(now, busy.get(link, 0.0)) if link else now
            busy[link] = begin + t
            tell(m, begin + t + under_way)
    assert len(order) == len(steps)
    return order


def arrived(ref, sem):
    pltpu.make_async_copy(ref, ref, sem).wait()


def bucket_kernel(
    rows_held, expert_hbm, weight_hbm, token_hbm, code_ref, share_ref, token_ref, expert_ref, weight_ref, load_sem
):
    loads = [
        pltpu.make_async_copy(src, dst, load_sem.at[i])
        for i, (src, dst) in enumerate(((expert_hbm, expert_ref), (weight_hbm, weight_ref), (token_hbm, token_ref)))
    ]
    for load in loads:
        load.start()
    slots, toks = expert_ref.shape
    ring, _, cap = code_ref.shape
    owners = ring * ring
    shift = rows_held.bit_length() - 1
    owner_no = lax.broadcasted_iota(I32, (owners, toks), 0)
    rank_no = lax.broadcasted_iota(I32, (cap, toks), 0)
    token_no = lax.broadcasted_iota(I32, (1, toks), 1).astype(F32)
    first = lax.broadcasted_iota(I32, (toks, toks), 0)
    second = lax.broadcasted_iota(I32, (toks, toks), 1)
    earlier = jnp.where(first < second, 1.0, 0.0).astype(BF16)
    ones = jnp.ones((toks, 128), BF16)
    for load in loads:
        load.wait()
    experts = [expert_ref[k : k + 1, :] for k in range(slots)]
    mine = [(expert >> shift) == owner_no for expert in experts]
    onehot = jnp.concatenate([jnp.where(m, 1.0, 0.0).astype(BF16) for m in mine], axis=0)
    ahead = jnp.dot(onehot, earlier, preferred_element_type=F32)
    total = jnp.dot(onehot, ones, preferred_element_type=F32)
    before = jnp.zeros((owners, ones.shape[1]), F32)
    what, where = [], []
    for k in range(slots):
        rows = slice(k * owners, (k + 1) * owners)
        rank = ahead[rows] + jnp.concatenate([before] * (toks // ones.shape[1]), axis=1)
        before = before + total[rows]
        rank = jnp.sum(jnp.where(mine[k], rank, 0.0), axis=0, keepdims=True).astype(I32)
        where.append(jnp.where(rank == rank_no, 1.0, 0.0).astype(BF16))
        local = experts[k] & (rows_held - 1)
        weight = weight_ref[k : k + 1, :]
        weight_hi = weight.astype(BF16).astype(F32)
        pieces = (
            (local >> 8).astype(F32),
            (local & 255).astype(F32),
            token_no,
            weight_hi,
            weight - weight_hi,
        )
        what.append(jnp.concatenate([jnp.where(mine[k], p, 0.0).astype(BF16) for p in pieces], axis=0))
    found = lax.dot_general(
        jnp.concatenate(what, axis=1), jnp.concatenate(where, axis=1), CONTRACT_MINOR, preferred_element_type=F32
    )
    part = [found[i * owners : (i + 1) * owners] for i in range(5)]
    code = part[2] * float(rows_held) + part[0] * 256.0 + part[1]
    weight = part[3] + part[4]
    for k in range(ring):
        code_ref[k] = code[k * ring : (k + 1) * ring].astype(I32)
        share_ref[k] = weight[k * ring : (k + 1) * ring]


def kernel(ring, *refs):
    messages = 2 * CHUNKS * ring * ring
    dma = pltpu.SemaphoreType.DMA
    pl.run_scoped(
        functools.partial(inside, ring, *refs),
        load_sem=dma((3,)),
        feat_sem=dma((messages,)),
        middle_sem=dma((2, ring)),
        pack_sem=dma((2, ring)),
        row_sem=dma,
        dot_sem=dma((CHUNKS * BATCHES,)),
        sum_sem=dma((messages,)),
        square_sem=dma((CHUNKS,)),
        sent_sem=dma((8,)),
    )


def inside(
    ring,
    n_tp,
    token_ref,
    code_ref,
    share_ref,
    up_ref,
    out_ref,
    gain_hbm,
    normed_ref,
    feats,
    gain_ref,
    staged,
    table,
    pair,
    code_middle,
    code_onward,
    code_packs,
    share_middle,
    share_onward,
    share_packs,
    codes,
    shares,
    tokens,
    row_vmem,
    row_smem,
    ups,
    outs,
    dots,
    dot_box,
    coefs,
    parts,
    inbox,
    inbox_x,
    inbox2,
    outbox,
    mixed,
    squares,
    *,
    load_sem,
    feat_sem,
    middle_sem,
    pack_sem,
    row_sem,
    dot_sem,
    sum_sem,
    square_sem,
    sent_sem,
):
    blocks = ring * ring
    held, width = up_ref.shape
    rows = feats.shape[1]
    span = 2 * rows
    cap = codes.shape[1]
    order = wave(ring)
    number = {uv: i for i, uv in enumerate(order)}
    me, mine = lax.axis_index("ep"), lax.axis_index("tp")
    z, y = me // ring, lax.rem(me, ring)
    turn = lambda k, by: lax.rem(k + by % ring, ring)
    column = lambda by: {"ep": turn(z, by) * ring + y}
    line = lambda by: {"ep": z * ring + turn(y, by)}
    across = lambda by: {"tp": lax.rem(mine + by, n_tp)}
    along = (column, line)
    place = lambda h, q, p: number[(q, p) if h == 0 else (p, q)]
    slot = lambda c, h, q, p: (c * 2 + h) * blocks + place(h, q, p)

    def remote(src, dst, sent, landed, device):
        pltpu.make_async_remote_copy(
            src, dst, sent, landed, device_id=device, device_id_type=MESH
        ).start()

    loads = [
        pltpu.make_async_copy(src, dst, load_sem.at[i])
        for i, (src, dst) in enumerate(
            ((up_ref, staged.at[0]), (out_ref, staged.at[1]), (gain_hbm, gain_ref))
        )
    ]
    for load in loads:
        load.start()
    barrier = pltpu.get_barrier_semaphore()
    peers = [f(by) for f in along for by in range(1, ring)] + [across(by) for by in range(1, n_tp)]
    for peer in peers:
        pl.semaphore_signal(barrier, inc=1, device_id=peer, device_id_type=MESH)

    steps, actions = {}, {}

    def step(name, time, needs, sends, action):
        steps[name] = (time, needs, sends)
        actions[name] = action

    wire = WIRE * 2 / CHUNKS

    def pass_on(c, h, q, p):
        here = slot(c, h, q, p)
        hops = [(h, way, slot(c, h, (q + way) % ring, 0)) for way in beyond(ring, q, h == 0) if p == 0]
        hops += [(1 - h, way, slot(c, h, q, (p + way) % ring)) for way in beyond(ring, p, q % 2 == 0)]

        def action():
            if (q, p) == (0, 0):
                source = token_ref.at[pl.ds((c * 2 + h) * rows, rows)]
                feats[here] = source[...]
            else:
                source = feats.at[here]
                arrived(source, feat_sem.at[here])
            for axis, way, there in hops:
                remote(source, feats.at[there], sent_sem.at[0], feat_sem.at[there], along[axis](way))

        needs = [] if (q, p) == (0, 0) else [("feat", here)]
        sends = [((axis, way), wire, HOP[axis, way], ("feat", there)) for axis, way, there in hops]
        step(("pass", c, h, q, p), 0.02, needs, sends, action)

    for c in range(CHUNKS):
        for h in range(2):
            for q, p in order:
                pass_on(c, h, q, p)

    parcels = (
        (code_ref, code_middle, code_onward, code_packs, codes),
        (share_ref, share_middle, share_onward, share_packs, shares),
    )

    def send_parcels():
        for kind, (parcel, middle, _, _, _) in enumerate(parcels):
            for by in far_first(ring):
                remote(parcel.at[turn(z, by)], middle.at[by], sent_sem.at[1 + kind], middle_sem.at[kind, by], column(by))
            middle[0] = parcel[z]

    def forward_parcels():
        for kind, (_, middle, onward, packs, _) in enumerate(parcels):
            for by in range(1, ring):
                arrived(middle.at[by], middle_sem.at[kind, by])
            for k in range(ring):
                for u in range(ring):
                    onward[k, u : u + 1, :] = middle[u, k : k + 1, :]
            for by in far_first(ring):
                remote(onward.at[turn(y, by)], packs.at[by], sent_sem.at[3 + kind], pack_sem.at[kind, by], line(by))
            packs[0] = onward[y]

    def open_packs():
        for kind, (_, _, _, packs, listed) in enumerate(parcels):
            for by in range(1, ring):
                arrived(packs.at[by], pack_sem.at[kind, by])
            for i, (u, v) in enumerate(order):
                listed[i : i + 1, :] = packs[v, u : u + 1, :]
        code = codes[...]
        row_vmem[...] = (code & (held - 1)) * 2
        tokens[...] = (code >> (held.bit_length() - 1)).astype(F32)

    fetch = pltpu.make_async_copy(row_vmem, row_smem, row_sem)
    letters = lambda axis, what: [((axis, way), 0.7, LETTER, (what, way)) for way in (1, -1)]
    step("send_parcels", 0.05, [], letters(0, "middle"), send_parcels)
    step("forward_parcels", 0.1, [("middle", 1), ("middle", -1)], letters(1, "pack"), forward_parcels)
    step("open_packs", 0.08, [("pack", 1), ("pack", -1)], [(None, 0.0, 0.1, "listed")], open_packs)
    step("fetch_rows", 0.02, ["listed"], [(None, 0.0, 1.1, "fetched")], fetch.start)
    step("rows", 0.01, ["fetched"], [], fetch.wait)

    def build_table():
        for load in loads:
            load.wait()
        for i in range(2):
            table[pl.ds(i, held, stride=2), :] = staged[i].astype(F32)

    step("build_table", 0.3, [], [], build_table)

    def gather(start):
        for i in range(start, start + GATHERS):
            both = pair.at[i % 2]
            for r in range(cap):
                both[2 * r : 2 * r + 2, :] = table[pl.ds(row_smem[i, r], 2), :]
            ups[i] = both[pl.ds(0, cap, stride=2), :].astype(BF16)
            outs[i] = both[pl.ds(1, cap, stride=2), :].astype(BF16)

    for i in range(0, blocks, GATHERS):
        step(("gather", i), PICK, ["rows", "build_table"], [], functools.partial(gather, i))

    batch = blocks // BATCHES
    sublane = lax.broadcasted_iota(I32, (8, cap), 0).astype(F32)
    token = lax.broadcasted_iota(I32, (span, cap), 0).astype(F32)

    def take_dots(c, b):
        def one(i):
            feat = jnp.concatenate([feats[(c * 2 + h) * blocks + i] for h in range(2)], axis=0)
            every = lax.dot_general(feat, ups[i], CONTRACT_MINOR, preferred_element_type=F32)
            here = tokens[i : i + 1, :] - (sublane + float(c * span))
            sums = [None] * 4
            for g in range(span // 8):
                term = jnp.where(here == float(8 * g), every[8 * g : 8 * g + 8, :], 0.0)
                sums[g % 4] = term if sums[g % 4] is None else sums[g % 4] + term
            total = (sums[0] + sums[1]) + (sums[2] + sums[3])
            dots[c, i : i + 1, :] = jnp.sum(total, axis=0, keepdims=True)

        for i in range(b * batch, (b + 1) * batch):
            one(i)
        some = pl.ds(b * batch, batch)
        for by in far_first(n_tp):
            remote(
                dots.at[c, some], dot_box.at[c, by, some], sent_sem.at[5], dot_sem.at[c * BATCHES + b], across(by)
            )

    def take_coefs(c, b):
        low, high = b * batch, (b + 1) * batch
        arrived(dot_box.at[c, pl.ds(1, n_tp - 1), pl.ds(low, batch)], dot_sem.at[c * BATCHES + b])
        total = dots[c, low:high, :]
        for by in range(1, n_tp):
            total = total + dot_box[c, by, low:high]
        coefs[c, low:high, :] = jax.nn.gelu(total) * shares[low:high, :]

        def one(i):
            here = tokens[i : i + 1, :] - float(c * span) == token
            coef = coefs[c, i : i + 1, :]
            coef_hi = coef.astype(BF16).astype(F32)
            spread = jnp.concatenate(
                [jnp.where(here, x, 0.0).astype(BF16) for x in (coef_hi, coef - coef_hi)], axis=1
            )
            both = jnp.concatenate([outs[i]] * 2, axis=0)
            parts[c, i] = jnp.dot(spread, both, preferred_element_type=F32)

        for i in range(b * batch, (b + 1) * batch):
            one(i)

    each = 0.66 / CHUNKS
    for c in range(CHUNKS):
        for b in range(BATCHES):
            mine_of = range(b * batch, (b + 1) * batch)
            needs = [("gather", i) for i in mine_of if i % GATHERS == 0]
            needs += [("pass", c, h, *order[i][:: 1 - 2 * h]) for i in mine_of for h in range(2)]
            sends = [(("x",), 0.175 * batch, ACROSS, ("totals", c, b))]
            step(("dots", c, b), each, needs, sends, functools.partial(take_dots, c, b))
            step(("mix", c, b), each, [("totals", c, b)], [], functools.partial(take_coefs, c, b))

    numbers = {}

    def box(*key):
        sem = sum_sem.at[numbers.setdefault(key, len(numbers))]
        kind, c, h, q, p, way = key
        if kind == 3:
            return inbox2.at[(c * 2 + h) * (ring + 3) + ring + (1 if q < ring // 2 else 2)], sem
        if kind == 1:
            if p == 0 and way < 0:
                return inbox_x.at[(c * 2 + h) * ring + q], sem
            return inbox.at[slot(c, h, q, p)], sem
        return inbox2.at[(c * 2 + h) * (ring + 3) + (ring if q == 0 and way < 0 else q)], sem

    def add_up(c, h, q, p):
        here = slot(c, h, q, p)
        plus = q % 2 == 0
        came = [(1, c, h, q, p, way if p == 0 else 0) for way in beyond(ring, p, plus)]
        straight = c == CHUNKS - 1
        far = 1
        if p == 0 and not (straight and distance(ring, q) == 1):
            came += [(2, c, h, q, 0, way if q == 0 else 0) for way in beyond(ring, q, h == 0)]
        if straight and (q, p) == (0, 0):
            came += [(3, c, h, k, 0, 0) for k in (2, ring - 2)]
        if p:
            way, axis = heading(ring, p, plus), 1 - h
            after = (p - way) % ring
            target = (1, c, h, q, after, way if after == 0 else 0)
        elif q:
            way, axis = heading(ring, q, h == 0), h
            after = (q - way) % ring
            target = (2, c, h, after, 0, way if after == 0 else 0)
            if straight and distance(ring, q) == 2:
                target, far = (3, c, h, q, 0, 0), 2
        else:
            target = None

        def action():
            value = parts[c, place(h, q, p), h * rows : (h + 1) * rows]
            for key in came:
                ref, sem = box(*key)
                arrived(ref, sem)
                value = value + ref[...].astype(F32)
            if target is None:
                mixed[c, h * rows : (h + 1) * rows] = value
                return
            outbox[here] = value.astype(BF16)
            ref, sem = box(*target)
            remote(outbox.at[here], ref, sent_sem.at[6], sem, along[axis](-way * far))

        needs = [("mix", c, place(h, q, p) // batch)] + [("sum", *key) for key in came]
        sends = [((axis, -way), wire * far, HOP[axis, -way] + 0.75 * (far - 1), ("sum", *target))] if target else []
        step(("add", c, h, q, p), 0.045, needs, sends, action)

    for c in range(CHUNKS):
        for h in range(2):
            for q, p in order:
                add_up(c, h, q, p)

    def send_squares(c):
        square = mixed[c] * mixed[c]
        square_hi = square.astype(BF16).astype(F32)
        split = jnp.concatenate([square_hi.astype(BF16), (square - square_hi).astype(BF16)], axis=1)
        ones = jnp.ones((8, 2 * width), BF16)
        sums = lax.dot_general(ones, split, CONTRACT_MINOR, preferred_element_type=F32)
        squares[c, 0] = sums[:1]
        for by in far_first(n_tp):
            remote(squares.at[c, 0], squares.at[c, by], sent_sem.at[7], square_sem.at[c], across(by))

    def finish(c):
        arrived(squares.at[c, pl.ds(1, n_tp - 1)], square_sem.at[c])
        total = squares[c, 0]
        for by in range(1, n_tp):
            total = total + squares[c, by]
        scale = lax.rsqrt(total / (width * n_tp) + 1e-06)
        same = lax.broadcasted_iota(I32, (span, span), 0) == lax.broadcasted_iota(I32, (span, span), 1)
        scales = jnp.sum(jnp.where(same, scale, 0.0), axis=1, keepdims=True)
        normed_ref[c * span : (c + 1) * span, :] = (mixed[c] * scales * gain_ref[...]).astype(BF16)

    for c in range(CHUNKS):
        needs = [("add", c, h, 0, 0) for h in range(2)]
        step(("square", c), 0.2, needs, [(("x",), 0.4, ACROSS, ("squares", c))], functools.partial(send_squares, c))
        step(("norm", c), 0.3, [("squares", c)], [], functools.partial(finish, c))

    def late(name):
        if isinstance(name, str):
            return -5
        kind, k = name[:2]
        if kind in ("square", "norm"):
            return -20
        wait = -SOONER[kind, 0 if kind == "gather" else k]
        if kind == "gather":
            return wait + NEXT_BATCH * (k // batch)
        return wait + NEXT_BATCH * name[2] * 0.5 if kind in ("dots", "mix") else wait

    plan = schedule(steps, SLACK, late)
    with scope("barrier"):
        pl.semaphore_wait(barrier, len(peers))
    for name in plan:
        with scope(name if isinstance(name, str) else "_".join(map(str, name))):
            actions[name]()

    with scope("drain"):
        sums = CHUNKS * 2 * (blocks - 1)
        arrived(feats.at[pl.ds(0, sums)], sent_sem.at[0])
        for kind, (_, middle, _, packs, _) in enumerate(parcels):
            arrived(middle.at[pl.ds(1, ring - 1)], sent_sem.at[1 + kind])
            arrived(packs.at[pl.ds(1, ring - 1)], sent_sem.at[3 + kind])
        arrived(dot_box.at[:, pl.ds(1, n_tp - 1)], sent_sem.at[5])
        arrived(outbox.at[pl.ds(0, sums)], sent_sem.at[6])
        arrived(squares.at[:, pl.ds(1, n_tp - 1)], sent_sem.at[7])


def body(tokens, experts, weights, up_table, out_table, gain):
    n_ep, n_tp = lax.axis_size("ep"), lax.axis_size("tp")
    ring = round(n_ep**0.5)
    toks, width = tokens.shape
    slots = experts.shape[1]
    held = up_table.shape[0]
    cap = 2 * toks * slots // n_ep
    rows = toks // (2 * CHUNKS)
    blocks = 2 * CHUNKS * n_ep
    hbm, vmem = pl.BlockSpec(memory_space=pltpu.HBM), pl.BlockSpec(memory_space=pltpu.VMEM)
    in_hbm = lambda x: pltpu.with_memory_space_constraint(x, pltpu.HBM)
    codes, shares, near_tokens = pl.pallas_call(
        functools.partial(bucket_kernel, held),
        out_shape=(
            jax.ShapeDtypeStruct((ring, ring, cap), I32),
            jax.ShapeDtypeStruct((ring, ring, cap), F32),
            jax.ShapeDtypeStruct((toks, width), BF16),
        ),
        in_specs=[hbm] * 3,
        out_specs=(vmem, vmem, vmem),
        scratch_shapes=[
            pltpu.VMEM((slots, toks), I32),
            pltpu.VMEM((slots, toks), F32),
            pltpu.SemaphoreType.DMA((3,)),
        ],
        compiler_params=pltpu.CompilerParams(vmem_limit_bytes=4 << 20),
        name="bucket",
    )(in_hbm(experts.T), in_hbm(weights.T), in_hbm(tokens))
    return pl.pallas_call(
        functools.partial(kernel, ring, n_tp),
        out_shape=jax.ShapeDtypeStruct((toks, width), BF16),
        in_specs=[vmem, vmem, vmem, hbm, hbm, hbm],
        out_specs=vmem,
        scratch_shapes=[
            pltpu.VMEM((blocks, rows, width), BF16),
            pltpu.VMEM((1, width), F32),
            pltpu.VMEM((2, held, width), BF16),
            pltpu.VMEM((2 * held, width), F32),
            pltpu.VMEM((2, 2 * cap, width), F32),
            pltpu.VMEM((ring, ring, cap), I32),
            pltpu.VMEM((ring, ring, cap), I32),
            pltpu.VMEM((ring, ring, cap), I32),
            pltpu.VMEM((ring, ring, cap), F32),
            pltpu.VMEM((ring, ring, cap), F32),
            pltpu.VMEM((ring, ring, cap), F32),
            pltpu.VMEM((n_ep, cap), I32),
            pltpu.VMEM((n_ep, cap), F32),
            pltpu.VMEM((n_ep, cap), F32),
            pltpu.VMEM((n_ep, cap), I32),
            pltpu.SMEM((n_ep, cap), I32),
            pltpu.VMEM((n_ep, cap, width), BF16),
            pltpu.VMEM((n_ep, cap, width), BF16),
            pltpu.VMEM((CHUNKS, n_ep, cap), F32),
            pltpu.VMEM((CHUNKS, n_tp, n_ep, cap), F32),
            pltpu.VMEM((CHUNKS, n_ep, cap), F32),
            pltpu.VMEM((CHUNKS, n_ep, 2 * rows, width), F32),
            pltpu.VMEM((blocks, rows, width), BF16),
            pltpu.VMEM((2 * CHUNKS * ring, rows, width), BF16),
            pltpu.VMEM((2 * CHUNKS * (ring + 3), rows, width), BF16),
            pltpu.VMEM((blocks, rows, width), BF16),
            pltpu.VMEM((CHUNKS, 2 * rows, width), F32),
            pltpu.VMEM((CHUNKS, n_tp, 1, 2 * rows), F32),
        ],
        compiler_params=pltpu.CompilerParams(
            collective_id=0, has_side_effects=True, vmem_limit_bytes=44 << 20
        ),
        name="retrieve",
    )(near_tokens, codes, shares, in_hbm(up_table), in_hbm(out_table), in_hbm(gain[None, :]))


def solution(mesh):
    placed = (P("ep", "tp"), P("ep", None), P("ep", None), P("ep", "tp"), P("ep", "tp"), P("tp"))
    return jax.shard_map(body, mesh=mesh, in_specs=placed, out_specs=P("ep", "tp"), check_vma=False)
```
